32 devices in a mesh: ep: 32 (over z, y, x, core).
Axes of the slice: x: 2, y: 2, z: 4, core: 2. Of those that a mesh axis runs over, the one named last changes fastest.
Arguments:
- tokens: bfloat16 [1024, 3072], P('ep'), may hold values from -6 to 6
- norm_gain: float32 [3072], replicated, may hold values from 0.1 to 1.9
- expert_ids: int32 [1024, 4], P('ep'), may hold values from 0 to 31, as said below
- expert_scores: float32 [1024, 4], P('ep'), may hold values from -100 to 180
- group_prob: float32 [1024], P('ep'), may hold values from 0.25 to 1
- gate_weight: bfloat16 [32, 3072, 384], P('ep'), may hold values from -0.109375 to 0.109375
- up_weight: bfloat16 [32, 3072, 384], P('ep'), may hold values from -0.109375 to 0.109375
- down_weight: bfloat16 [32, 384, 3072], P('ep'), may hold values from -0.3125 to 0.3125
Outputs:
- combined: bfloat16 [1024, 3072], P('ep')
The draws below stay inside these ranges and needn't reach their ends.
Inputs may be any that keep to these rules, and one draw needn't show every extreme that they name: `expert_ids`: the 4 ids of a row are different and lie in one group of 8 consecutive experts. Among the rows of one device no expert is named by more than 16 rows, and in every draw some expert is named by exactly 16 rows of one device.
All inputs are finite; a program needn't handle non-finite values.
Results may differ from the reference program's by a relative error of at most 0.0085.
Values may be sent and summed in bfloat16 or wider, within the bound.
A program may use at most 128 MiB of HBM per device.

```python
import jax
import jax.numpy as jnp
from jax import lax

D = 3072
FFE = 384
GROUPS = 4
TOP_K = 4
TOK_DEV = 32
EXPERTS = 32
TOKENS = 1024
MOST = 16
N_EP = 32


def draw_expert_ids(key, part):
    blocks_count = TOKENS // TOK_DEV
    group_size = EXPERTS // GROUPS
    hot_count = (MOST - 1) * group_size // TOP_K + 1
    keys = jax.random.split(jax.random.fold_in(key, 11), 5)
    group_order = jax.random.permutation(keys[0], GROUPS)
    chosen_rank = jnp.min(jax.random.randint(keys[1], (3, blocks_count, TOK_DEV), 0, GROUPS), axis=0)
    hot_rank = jnp.min(jax.random.randint(keys[2], (3, blocks_count, 1), 0, GROUPS), axis=0)
    position = jnp.arange(TOK_DEV)[None, :]
    group_index = group_order[jnp.where(position < hot_count, hot_rank, chosen_rank)]
    earlier_mask = (group_index[:, :, None] == group_index[:, None, :]) & (jnp.arange(TOK_DEV)[None, None, :] < jnp.arange(TOK_DEV)[None, :, None])
    earlier = jnp.sum(earlier_mask.astype(jnp.int32), axis=2)
    starts = jax.random.randint(keys[3], (blocks_count, GROUPS), 0, group_size)
    start_here = jnp.take_along_axis(starts, group_index, axis=1)
    local_ids = (start_here[:, :, None] + earlier[:, :, None] * TOP_K + jnp.arange(TOP_K)[None, None, :]) % group_size
    global_ids = group_index[:, :, None] * group_size + local_ids
    return global_ids.reshape(TOKENS, TOP_K).astype(jnp.int32)


def draw_expert_scores(key, part):
    keys = jax.random.split(jax.random.fold_in(key, 23), 3)
    base_scores = jnp.clip(jax.random.normal(keys[0], (TOKENS, TOP_K), jnp.float32), -6.0, 6.0) * 1.5
    return base_scores.astype(jnp.float32)


def levels(rng, dims, shards, low, high):
    def one(axis_at, parts):
        heights = jax.random.uniform(jax.random.fold_in(jax.random.fold_in(rng, 6), axis_at), (parts,), jnp.float32, low / len(shards), high / len(shards))
        return jnp.repeat(jnp.exp(heights), dims[axis_at] // parts).reshape((-1,) + (1,) * (len(dims) - axis_at - 1))

    level = one(*shards[0])
    for cut in shards[1:]:
        level = level * one(*cut)
    return level


def gaussian(key, dims, deviation, reach, shards=(), kind=jnp.bfloat16):
    drawn = deviation * jax.random.normal(key, dims, jnp.float32)
    if shards:
        drawn = drawn * levels(key, dims, shards, -0.22, 0.18)
    return jnp.clip(drawn, -reach, reach).astype(kind)


def setup_inputs(seed: int = 0) -> dict:
    streams_of = jax.random.split(jax.random.key(seed), 9)
    return {
        "tokens": gaussian(streams_of[0], (TOKENS, D), 1.0, 6.0, ((0, 32),)),
        "norm_gain": jnp.clip(1.0 + 0.18 * jax.random.normal(streams_of[1], (D,), jnp.float32), 0.1, 1.9),
        "expert_ids": draw_expert_ids(jax.random.fold_in(streams_of[8], 71), 0),
        "expert_scores": draw_expert_scores(jax.random.fold_in(streams_of[8], 71), 0),
        "group_prob": jnp.clip(0.25 + 0.75 * jax.random.uniform(streams_of[4], (TOKENS,), jnp.float32) ** levels(streams_of[4], (TOKENS,), ((0, 32),), -0.2, 0.2), 0.25, 1.0),
        "gate_weight": gaussian(streams_of[5], (EXPERTS, D, FFE), D ** -0.5, 0.109375, ((0, 32),)),
        "up_weight": gaussian(streams_of[6], (EXPERTS, D, FFE), D ** -0.5, 0.109375, ((0, 32),)),
        "down_weight": gaussian(streams_of[7], (EXPERTS, FFE, D), FFE ** -0.5, 0.3125, ((0, 32),)),
    }


eps_norm = 1e-05

def layer_norm(tokens, norm_gain):
    values = tokens.astype(jnp.float32)
    average = lax.optimization_barrier(jnp.mean(values, axis=1, keepdims=True))
    centred = values - average
    variance = lax.optimization_barrier(jnp.mean(centred * centred, axis=1, keepdims=True))
    return (centred * lax.rsqrt(variance + eps_norm) * norm_gain[None, :]).astype(jnp.bfloat16)

def mixing_weights(expert_scores, group_prob):
    shifted = expert_scores - lax.optimization_barrier(jnp.max(expert_scores, axis=1, keepdims=True))
    exp_scores = jnp.exp(shifted)
    return exp_scores / lax.optimization_barrier(jnp.sum(exp_scores, axis=1, keepdims=True)) * group_prob[:, None]

def expert_rows(flat_rows, gate_matrix, up_matrix, down_matrix):
    gate_act = jnp.dot(flat_rows, gate_matrix, preferred_element_type=jnp.float32)
    up_act = jnp.dot(flat_rows, up_matrix, preferred_element_type=jnp.float32)
    hidden = (jax.nn.silu(gate_act) * up_act).astype(jnp.bfloat16)
    return jnp.dot(hidden, down_matrix, preferred_element_type=jnp.float32).astype(jnp.bfloat16)

def reference(tokens, norm_gain, expert_ids, expert_scores, group_prob, gate_weight, up_weight, down_weight):
    normed = layer_norm(tokens, norm_gain)
    weights_tok = mixing_weights(expert_scores, group_prob)
    capacity = N_EP * MOST
    slot_iota = jnp.arange(capacity, dtype=jnp.int32)

    def per_expert(running, expert_index):
        matches = expert_ids == expert_index
        chosen = jnp.any(matches, axis=1)
        own_weight = lax.optimization_barrier(jnp.sum(jnp.where(matches, weights_tok, 0.0), axis=1))
        slot_token = jnp.nonzero(chosen, size=capacity, fill_value=0)[0].astype(jnp.int32)
        filled = slot_iota < jnp.sum(chosen.astype(jnp.int32))
        results = expert_rows(normed[slot_token], gate_weight[expert_index], up_weight[expert_index], down_weight[expert_index])
        slot_scale = jnp.where(filled, own_weight[slot_token], 0.0)
        running = running.at[slot_token].add(slot_scale[:, None] * results.astype(jnp.float32))
        return (running, None)
    start = jnp.zeros((TOKENS, D), jnp.float32)
    mixture, _ = lax.scan(per_expert, start, jnp.arange(EXPERTS, dtype=jnp.int32))
    return mixture.astype(jnp.bfloat16)
```

```python
import functools

import jax
import jax.numpy as jnp
from jax import lax
from jax.experimental import pallas as pl
from jax.experimental.pallas import tpu as pltpu
from jax.sharding import PartitionSpec as P

GROUPS = 4
TOP_K = 4
LANES = 128
MESH = pl.DeviceIdType.MESH


eps_norm = 1e-05


def layer_norm(tokens, norm_gain):
    values = tokens.astype(jnp.float32)
    average = jnp.mean(values, axis=1, keepdims=True)
    centred = values - average
    variance = jnp.mean(centred * centred, axis=1, keepdims=True)
    return (centred * lax.rsqrt(variance + eps_norm) * norm_gain[None, :]).astype(jnp.bfloat16)


def mixing_weights(expert_scores, group_prob):
    shifted = expert_scores - jnp.max(expert_scores, axis=1, keepdims=True)
    exp_scores = jnp.exp(shifted)
    return exp_scores / jnp.sum(exp_scores, axis=1, keepdims=True) * group_prob[:, None]


def expert_rows(flat_rows, gate_matrix, up_matrix, down_matrix):
    gate_act = jnp.dot(flat_rows, gate_matrix, preferred_element_type=jnp.float32)
    up_act = jnp.dot(flat_rows, up_matrix, preferred_element_type=jnp.float32)
    hidden = (jax.nn.silu(gate_act) * up_act).astype(jnp.bfloat16)
    return jnp.dot(hidden, down_matrix, preferred_element_type=jnp.float32).astype(jnp.bfloat16)


def local(
    tokens, norm_gain, expert_ids, expert_scores, group_prob, gate_weight, up_weight, down_weight
):
    normed = layer_norm(tokens, norm_gain)
    weights_tok = mixing_weights(expert_scores, group_prob)
    tok_count = tokens.shape[0]
    model_width = tokens.shape[1]
    expert_count = lax.axis_size("ep")
    group_size = expert_count // GROUPS
    capacity = (tok_count * TOP_K + group_size - 1) // group_size
    expert_iota = jnp.arange(expert_count, dtype=jnp.int32)
    slot_iota = jnp.arange(capacity, dtype=jnp.int32)
    matches = expert_ids[:, :, None] == expert_iota[None, None, :]
    route_weight = jnp.sum(jnp.where(matches, weights_tok[:, :, None], 0.0), axis=1)
    gate_matrix = gate_weight[0]
    up_matrix = up_weight[0]
    down_matrix = down_weight[0]
    chosen = jnp.sum(matches.astype(jnp.int32), axis=1)
    order_rank = jnp.cumsum(chosen, axis=0) - chosen
    slot_map = (chosen.T[:, None, :] == 1) & (order_rank.T[:, None, :] == slot_iota[None, :, None])
    outgoing = jnp.einsum(
        "emt,td->emd", slot_map.astype(jnp.bfloat16), normed, preferred_element_type=jnp.float32
    ).astype(jnp.bfloat16)
    received = lax.all_to_all(outgoing, "ep", split_axis=0, concat_axis=0, tiled=True)
    flat_rows = received.reshape(-1, model_width)
    results = expert_rows(flat_rows, gate_matrix, up_matrix, down_matrix).reshape(received.shape)
    returned_rows = lax.all_to_all(results, "ep", split_axis=0, concat_axis=0, tiled=True)
    slot_scale = jnp.where(slot_map, route_weight.T[:, None, :], 0.0)
    mixture = jnp.einsum(
        "emt,emd->td",
        slot_scale,
        returned_rows.astype(jnp.float32),
        precision=lax.Precision.HIGHEST,
    )
    return mixture.astype(jnp.bfloat16)

CHUNKS = 4


def plan():
    order = []

    def at(time, *step):
        order.append((time, len(order), step))

    for k in range(CHUNKS):
        base = 6.3 * k
        at(max(base - 4.0, 0.1 * k), "own", k)
        at(base + 2.5, "first", k)
        for i in range(1, 4):
            at(base + 2.5 + 2.3 * i, "line", k, i)
        for i in range(4):
            at(base + 4.9 + 2.3 * i, "last", k, i)
        ready = base + 14.0
        at(ready, "hidden", k)
        at(ready + 1.5, "down", k)
        at(ready + 4.0, "back", k)
        for i in range(3):
            at(ready + 7.5 + 2.3 * i, "sum", k, i)
        at(ready + 14.5, "home", k)
        at(ready + 17.0, "final", k)
        at(ready + 8.0, "drain_out", k)
        at(ready + 20.0, "drain_back", k)
    return [step for _, _, step in sorted(order)]


def ring_kernel(
    zs, tok_ref, gain_ref, ids_ref, score_ref, prob_ref, gate_hbm, up_hbm, down_hbm, out_ref,
    xg, stage, part, pair_in, last_in, line_in, first_in, fin_in, hid, scales, wgu, wd, w_sem,
    stage_send, stage_recv, gather_recv, own_send, first_send, line_send, last_send,
    mate_send, mate_recv, pair_send, pair_recv, back_send, back_recv, sum_send, sum_recv,
    home_send, home_recv, fin_send, fin_recv,
):
    me = lax.axis_index("ep")
    core = lax.rem(me, 2)
    x = lax.rem(lax.div(me, 2), 2)
    y = lax.rem(lax.div(me, 4), 2)
    z = lax.div(me, 8)
    other = 1 - core

    def device(zz, yy, xx, cc):
        return ((zz * 2 + yy) * 2 + xx) * 2 + cc

    partner = device(z, y, x, other)
    first_dev = device(z, y + core * (1 - 2 * y), x + other * (1 - 2 * x), core)
    last_dev = device(z, y + other * (1 - 2 * y), x + core * (1 - 2 * x), core)
    has = (z > 0, z < zs - 1)

    def column(fr, lr):
        dx = other * fr + core * lr
        dy = core * fr + other * lr
        xx = x + dx * (1 - 2 * x)
        yy = y + dy * (1 - 2 * y)
        return (xx * 2 + yy) * zs

    cols = [[column(fr, lr) for lr in (0, 1)] for fr in (0, 1)]
    near = [sorted(range(zs), key=lambda q, zz=zz: (abs(q - zz), -q if zz < zs // 2 else q))
            for zz in range(zs)]
    planes = []
    for i in range(zs):
        q = jnp.int32(near[0][i])
        for zz in range(1, zs):
            q = jnp.where(z == zz, near[zz][i], q)
        planes.append(q)
    below = [q < z for q in planes]
    away = [jnp.where(b, z + 1, z - 1) for b in below]
    away_ok = [jnp.logical_and(a >= 0, a < zs) for a in away]
    toward = [jnp.where(b, z - 1, z + 1) for b in below]
    side_of = [jnp.where(b, 1, 0) for b in below]

    model_width = tok_ref.shape[1]
    half = model_width // 2
    count = tok_ref.shape[0]
    rows = stage.shape[1]
    blocks = 4 * zs

    copies = [
        pltpu.make_async_copy(gate_hbm.at[0], wgu.at[:, : wgu.shape[1] // 2], w_sem.at[0]),
        pltpu.make_async_copy(up_hbm.at[0], wgu.at[:, wgu.shape[1] // 2 :], w_sem.at[1]),
        pltpu.make_async_copy(down_hbm.at[0, :, :half], wd.at[0], w_sem.at[2]),
        pltpu.make_async_copy(down_hbm.at[0, :, half:], wd.at[1], w_sem.at[3]),
    ]
    for copy in copies:
        copy.start()

    barrier = pltpu.get_barrier_semaphore()
    for peer in (partner, first_dev, last_dev):
        pl.semaphore_signal(barrier, inc=1, device_id=(peer,), device_id_type=MESH)
    for d in (0, 1):
        @pl.when(has[d])
        def _():
            pl.semaphore_signal(
                barrier, inc=1, device_id=(device(z - 1 + 2 * d, y, x, core),), device_id_type=MESH
            )

    def remote(src, dst, send_sem, recv_sem, target):
        return pltpu.make_async_remote_copy(
            src_ref=src, dst_ref=dst, send_sem=send_sem, recv_sem=recv_sem,
            device_id=(target,), device_id_type=MESH,
        )

    def landed(ref, sem):
        remote(ref, ref, sem, sem, partner).wait_recv()

    def sent(ref, sem):
        remote(ref, ref, sem, sem, partner).wait_send()

    def wide(k):
        return half + LANES if k == 0 else half

    def block(h, k, slot):
        return xg.at[h, k, slot, :, pl.ds(0, wide(k))]

    def span(h, k, n):
        return xg.at[h, k, pl.ds(0, n), :, pl.ds(0, wide(k))]

    own_slot = cols[0][0] + z

    values = tok_ref[...].astype(jnp.float32)
    average = jnp.sum(values, axis=1, keepdims=True) * (1.0 / model_width)
    centred = values - average
    variance = jnp.sum(centred * centred, axis=1, keepdims=True) * (1.0 / model_width)
    normed = (centred * lax.rsqrt(variance + eps_norm) * gain_ref[...]).astype(jnp.bfloat16)
    for c in (0, 1):
        @pl.when(core == c)
        def _():
            for j in range(CHUNKS // 2):
                piece = normed[j * rows : (j + 1) * rows]
                mine = piece[:, :half] if c == 0 else piece[:, half:]
                theirs = piece[:, half:] if c == 0 else piece[:, :half]
                xg[c, 2 * j + c, own_slot, :, :half] = mine
                stage[j] = theirs
    score = [score_ref[k : k + 1, :] for k in range(TOP_K)]
    top = functools.reduce(jnp.maximum, score)
    exps = [jnp.exp(s - top) for s in score]
    total = functools.reduce(jnp.add, exps)
    row = lax.broadcasted_iota(jnp.int32, (rows, count), 0)
    tags = jnp.zeros((rows, count), jnp.float32)
    for k in range(TOP_K):
        weight = exps[k] / total * prob_ref[...]
        high = weight.astype(jnp.bfloat16).astype(jnp.float32)
        tags = jnp.where(row == k, ids_ref[k : k + 1, :].astype(jnp.float32), tags)
        tags = jnp.where(row == TOP_K + k, high, tags)
        tags = jnp.where(row == 2 * TOP_K + k, weight - high, tags)
    tags = jnp.concatenate([tags, jnp.zeros((rows, LANES - count), jnp.float32)], axis=1)
    xg[core, 0, own_slot, :, half:] = tags.astype(jnp.bfloat16)

    inside = jnp.logical_and(has[0], has[1])

    @pl.when(inside)
    def _():
        pl.semaphore_wait(barrier, 5)

    @pl.when(jnp.logical_not(inside))
    def _():
        pl.semaphore_wait(barrier, 4)

    for j in range(CHUNKS // 2):
        k = 2 * j + core
        remote(stage.at[j], xg.at[core * 0 + other, k, own_slot, :, pl.ds(0, half)],
               stage_send.at[j], stage_recv.at[k], partner).start()

    def spread(k, slot, fr, i):
        ref = block(core, k, slot)
        sem = gather_recv.at[k, slot]
        if i == 0:
            for d in (0, 1):
                @pl.when(has[d])
                def _():
                    remote(ref, ref, own_send.at[k, d], sem, device(z - 1 + 2 * d, y, x, core)).start()
        else:
            @pl.when(away_ok[i])
            def _():
                remote(ref, ref, line_send.at[k, i], sem, device(away[i], y, x, core)).start()
        remote(ref, ref, last_send.at[k], sem, last_dev).start()
        remote(ref, ref, mate_send.at[k], mate_recv.at[k], partner).start()

    def own(k):
        @pl.when(core != k % 2)
        def _():
            landed(xg.at[core, k, own_slot, :, pl.ds(0, half)], stage_recv.at[k])
        ref = block(core, k, own_slot)
        remote(ref, ref, first_send.at[k], gather_recv.at[k, own_slot], first_dev).start()
        spread(k, own_slot, 0, 0)

    def first(k):
        slot = cols[1][0] + z
        landed(block(core, k, slot), gather_recv.at[k, slot])
        spread(k, slot, 1, 0)

    def line(k, i):
        for fr in (0, 1):
            slot = cols[fr][0] + planes[i]
            landed(block(core, k, slot), gather_recv.at[k, slot])
            spread(k, slot, fr, i)

    def last(k, i):
        for fr in (0, 1):
            slot = cols[fr][1] + planes[i]
            ref = block(core, k, slot)
            landed(ref, gather_recv.at[k, slot])
            remote(ref, ref, mate_send.at[k], mate_recv.at[k], partner).start()

    def hidden(k):
        landed(span(other, k, blocks), mate_recv.at[k])
        if k == 0:
            for copy in copies:
                copy.wait()
            expert = me.astype(jnp.float32)
            for h in (0, 1):
                tags = xg[h, 0, :, :, half:].astype(jnp.float32)
                scale = jnp.zeros((blocks, LANES), jnp.float32)
                for n in range(TOP_K):
                    value = tags[:, TOP_K + n, :] + tags[:, 2 * TOP_K + n, :]
                    scale += jnp.where(tags[:, n, :] == expert, value, 0.0)
                scales[h] = scale
        shape = (blocks, rows, LANES)
        pick = lax.broadcasted_iota(jnp.int32, shape, 2) == (
            lax.broadcasted_iota(jnp.int32, shape, 1) + rows * (k // 2))
        scale = jnp.sum(jnp.where(pick, scales[k % 2][:, None, :], 0.0), axis=2, keepdims=True)
        scale = scale.reshape(blocks * rows, 1)
        left = xg[0, k, :, :, :half].reshape(blocks * rows, half)
        right = xg[1, k, :, :, :half].reshape(blocks * rows, half)
        acts = jnp.dot(left, wgu[:half, :], preferred_element_type=jnp.float32) + jnp.dot(
            right, wgu[half:, :], preferred_element_type=jnp.float32
        )
        inner = hid.shape[1]
        hid[...] = (jax.nn.silu(acts[:, :inner]) * acts[:, inner:] * scale).astype(jnp.bfloat16)

    def down(k):
        step = half // 3 if half % (3 * LANES) == 0 else half
        for h in (other, core):
            for at in range(0, half, step):
                out = jnp.dot(hid[...], wd[h, :, at : at + step], preferred_element_type=jnp.float32)
                part[h, k, :, :, at : at + step] = out.astype(jnp.bfloat16).reshape(blocks, rows, step)
            if h is other:
                remote(part.at[other, k], pair_in.at[k], pair_send.at[k], pair_recv.at[k], partner).start()

    def back(k):
        landed(pair_in.at[k], pair_recv.at[k])
        for i in range(zs - 1, -1, -1):
            for fr in (0, 1):
                slot = cols[fr][1] + planes[i]
                part[core, k, slot] = part[core, k, slot] + pair_in[k, slot]
                remote(part.at[core, k, slot], last_in.at[k, fr, planes[i]], back_send.at[k],
                       back_recv.at[k, fr, planes[i]], last_dev).start()

    def gathered(k, fr, q):
        slot = cols[fr][0] + q
        landed(last_in.at[k, fr, q], back_recv.at[k, fr, q])
        held = part[core, k, slot].astype(jnp.float32) + pair_in[k, slot].astype(jnp.float32)
        part[core, k, slot] = (held + last_in[k, fr, q].astype(jnp.float32)).astype(jnp.bfloat16)
        return slot

    def line_sum(k, j):
        i = zs - 1 - j
        q = planes[i]
        for fr in (0, 1):
            slot = gathered(k, fr, q)

            @pl.when(away_ok[i])
            def _():
                landed(line_in.at[k, side_of[i], fr, q], sum_recv.at[k, side_of[i], fr, q])
                part[core, k, slot] = part[core, k, slot] + line_in[k, side_of[i], fr, q]

            remote(part.at[core, k, slot], line_in.at[k, side_of[i], fr, q], sum_send.at[k],
                   sum_recv.at[k, side_of[i], fr, q], device(toward[i], y, x, core)).start()

    def home(k):
        for fr in (1, 0):
            slot = gathered(k, fr, z)
            for d in (0, 1):
                @pl.when(has[d])
                def _():
                    landed(line_in.at[k, d, fr, z], sum_recv.at[k, d, fr, z])
                    part[core, k, slot] = part[core, k, slot] + line_in[k, d, fr, z]
            if fr == 1:
                remote(part.at[core, k, slot], first_in.at[k], home_send.at[k], home_recv.at[k],
                       first_dev).start()

    def final(k):
        landed(first_in.at[k], home_recv.at[k])
        total = part[core, k, own_slot] + first_in[k]
        j = k // 2

        @pl.when(core == k % 2)
        def _():
            out_ref[j * rows : (j + 1) * rows, pl.ds(pl.multiple_of(core * half, LANES), half)] = total

        @pl.when(core != k % 2)
        def _():
            part[core, k, own_slot] = total
            remote(part.at[core, k, own_slot], fin_in.at[j], fin_send.at[j], fin_recv.at[j],
                   partner).start()

    def drain_out(k):
        @pl.when(core == k % 2)
        def _():
            sent(stage.at[k // 2], stage_send.at[k // 2])
        sent(block(core, k, own_slot), first_send.at[k])
        for d in (0, 1):
            @pl.when(has[d])
            def _():
                sent(span(core, k, 2), own_send.at[k, d])
        for i in range(1, zs):
            @pl.when(away_ok[i])
            def _():
                sent(span(core, k, 2), line_send.at[k, i])
        sent(span(core, k, 2 * zs), last_send.at[k])
        sent(span(core, k, blocks), mate_send.at[k])

    def drain_back(k):
        sent(part.at[other, k], pair_send.at[k])
        sent(part.at[core, k, pl.ds(0, 2 * zs)], back_send.at[k])
        sent(part.at[core, k, pl.ds(0, 2 * (zs - 1))], sum_send.at[k])
        sent(part.at[core, k, 0], home_send.at[k])

    steps = dict(own=own, first=first, line=line, last=last, hidden=hidden, down=down, back=back,
                 sum=line_sum, home=home, final=final, drain_out=drain_out, drain_back=drain_back)
    for name, *rest in plan():
        steps[name](*rest)

    for j in range(CHUNKS // 2):
        landed(fin_in.at[j], fin_recv.at[j])
        out_ref[j * rows : (j + 1) * rows, pl.ds(pl.multiple_of(other * half, LANES), half)] = fin_in[j]
    for j in range(CHUNKS // 2):
        sent(fin_in.at[j], fin_send.at[j])


def ring_local(
    zs, tokens, norm_gain, expert_ids, expert_scores, group_prob, gate_weight, up_weight, down_weight
):
    count, width = tokens.shape
    inner = gate_weight.shape[2]
    half = width // 2
    rows = 2 * count // CHUNKS
    blocks = 4 * zs
    kind = jnp.bfloat16
    vmem = pl.BlockSpec(memory_space=pltpu.VMEM)
    hbm = pl.BlockSpec(memory_space=pl.ANY)
    dma = pltpu.SemaphoreType.DMA
    c = CHUNKS
    scratch = [
        pltpu.VMEM((2, c, blocks, rows, half + LANES), kind),
        pltpu.VMEM((c // 2, rows, half), kind),
        pltpu.VMEM((2, c, blocks, rows, half), kind),
        pltpu.VMEM((c, blocks, rows, half), kind),
        pltpu.VMEM((c, 2, zs, rows, half), kind),
        pltpu.VMEM((c, 2, 2, zs, rows, half), kind),
        pltpu.VMEM((c, rows, half), kind),
        pltpu.VMEM((c // 2, rows, half), kind),
        pltpu.VMEM((blocks * rows, inner), kind),
        pltpu.VMEM((2, blocks, LANES), jnp.float32),
        pltpu.VMEM((width, 2 * inner), kind),
        pltpu.VMEM((2, inner, half), kind),
        dma((4,)),
        dma((c // 2,)), dma((c,)), dma((c, blocks)), dma((c, 2)), dma((c,)), dma((c, zs)), dma((c,)),
        dma((c,)), dma((c,)), dma((c,)), dma((c,)), dma((c,)), dma((c, 2, zs)),
        dma((c,)), dma((c, 2, 2, zs)),
        dma((c,)), dma((c,)), dma((c // 2,)), dma((c // 2,)),
    ]
    return pl.pallas_call(
        functools.partial(ring_kernel, zs),
        out_shape=jax.ShapeDtypeStruct((count, width), kind),
        in_specs=[vmem] * 5 + [hbm] * 3,
        out_specs=vmem,
        scratch_shapes=scratch,
        compiler_params=pltpu.CompilerParams(
            collective_id=0, has_side_effects=True, vmem_limit_bytes=60 * 1024 * 1024
        ),
    )(
        tokens, norm_gain[None, :], expert_ids.T, expert_scores.T, group_prob[None, :], gate_weight, up_weight, down_weight,
    )


def solution(mesh):
    in_specs = (
        P("ep", None),
        P(),
        P("ep", None),
        P("ep", None),
        P("ep"),
        P("ep", None, None),
        P("ep", None, None),
        P("ep", None, None),
    )
    out_specs = P("ep", None)
    devices = mesh.shape["ep"]
    body = functools.partial(ring_local, GROUPS) if devices == GROUPS * 8 else local
    return jax.shard_map(body, mesh=mesh, in_specs=in_specs, out_specs=out_specs, check_vma=False)
```

```python
import functools

import jax
import jax.numpy as jnp
from jax import lax
from jax.experimental import pallas as pl
from jax.experimental.pallas import tpu as pltpu
from jax.sharding import PartitionSpec as P

GROUPS = 4
TOP_K = 4
LANES = 128
MESH = pl.DeviceIdType.MESH


eps_norm = 1e-05


def layer_norm(tokens, norm_gain):
    values = tokens.astype(jnp.float32)
    average = jnp.mean(values, axis=1, keepdims=True)
    centred = values - average
    variance = jnp.mean(centred * centred, axis=1, keepdims=True)
    return (centred * lax.rsqrt(variance + eps_norm) * norm_gain[None, :]).astype(jnp.bfloat16)


def mixing_weights(expert_scores, group_prob):
    shifted = expert_scores - jnp.max(expert_scores, axis=1, keepdims=True)
    exp_scores = jnp.exp(shifted)
    return exp_scores / jnp.sum(exp_scores, axis=1, keepdims=True) * group_prob[:, None]


def expert_rows(flat_rows, gate_matrix, up_matrix, down_matrix):
    gate_act = jnp.dot(flat_rows, gate_matrix, preferred_element_type=jnp.float32)
    up_act = jnp.dot(flat_rows, up_matrix, preferred_element_type=jnp.float32)
    hidden = (jax.nn.silu(gate_act) * up_act).astype(jnp.bfloat16)
    return jnp.dot(hidden, down_matrix, preferred_element_type=jnp.float32).astype(jnp.bfloat16)


def local(
    tokens, norm_gain, expert_ids, expert_scores, group_prob, gate_weight, up_weight, down_weight
):
    normed = layer_norm(tokens, norm_gain)
    weights_tok = mixing_weights(expert_scores, group_prob)
    tok_count = tokens.shape[0]
    model_width = tokens.shape[1]
    expert_count = lax.axis_size("ep")
    group_size = expert_count // GROUPS
    capacity = (tok_count * TOP_K + group_size - 1) // group_size
    expert_iota = jnp.arange(expert_count, dtype=jnp.int32)
    slot_iota = jnp.arange(capacity, dtype=jnp.int32)
    matches = expert_ids[:, :, None] == expert_iota[None, None, :]
    route_weight = jnp.sum(jnp.where(matches, weights_tok[:, :, None], 0.0), axis=1)
    gate_matrix = gate_weight[0]
    up_matrix = up_weight[0]
    down_matrix = down_weight[0]
    chosen = jnp.sum(matches.astype(jnp.int32), axis=1)
    order_rank = jnp.cumsum(chosen, axis=0) - chosen
    slot_map = (chosen.T[:, None, :] == 1) & (order_rank.T[:, None, :] == slot_iota[None, :, None])
    outgoing = jnp.einsum(
        "emt,td->emd", slot_map.astype(jnp.bfloat16), normed, preferred_element_type=jnp.float32
    ).astype(jnp.bfloat16)
    received = lax.all_to_all(outgoing, "ep", split_axis=0, concat_axis=0, tiled=True)
    flat_rows = received.reshape(-1, model_width)
    results = expert_rows(flat_rows, gate_matrix, up_matrix, down_matrix).reshape(received.shape)
    returned_rows = lax.all_to_all(results, "ep", split_axis=0, concat_axis=0, tiled=True)
    slot_scale = jnp.where(slot_map, route_weight.T[:, None, :], 0.0)
    mixture = jnp.einsum(
        "emt,emd->td",
        slot_scale,
        returned_rows.astype(jnp.float32),
        precision=lax.Precision.HIGHEST,
    )
    return mixture.astype(jnp.bfloat16)

CHUNKS = 4


ORDER = (
    ("own", 2), ("own", 0), ("own", 1), ("first", 2), ("own", 3), ("first", 0), ("first", 1),
    ("line", 1, 1, 0), ("line", 0, 1, 0), ("first", 3), ("line", 0, 2, 0), ("line", 1, 1, 1),
    ("line", 1, 2, 1), ("last", 0, 2, 0), ("line", 0, 1, 1), ("line", 0, 3, 0), ("last", 1, 1, 0),
    ("line", 0, 2, 1), ("last", 0, 0, 0), ("last", 0, 1, 0), ("line", 2, 1, 0), ("last", 0, 0, 1),
    ("line", 0, 3, 1), ("line", 1, 2, 0), ("line", 1, 3, 1), ("last", 0, 2, 1), ("last", 1, 1, 1),
    ("last", 1, 0, 0), ("last", 0, 1, 1), ("last", 1, 2, 1), ("last", 0, 3, 0), ("line", 2, 1, 1),
    ("last", 2, 0, 0), ("line", 2, 2, 1), ("last", 1, 0, 1), ("last", 3, 0, 0), ("last", 0, 3, 1),
    ("line", 1, 3, 0), ("line", 3, 2, 0), ("line", 2, 2, 0), ("line", 3, 1, 0), ("last", 1, 3, 1),
    ("hidden", 0), ("line", 2, 3, 1), ("last", 1, 3, 0), ("line", 3, 1, 1), ("last", 1, 2, 0),
    ("last", 2, 2, 1), ("down", 0), ("last", 2, 1, 1), ("last", 2, 1, 0), ("line", 2, 3, 0),
    ("line", 3, 2, 1), ("hidden", 1), ("last", 2, 0, 1), ("last", 2, 3, 1), ("back", 0), ("down", 1),
    ("line", 3, 3, 1), ("last", 2, 2, 0), ("last", 2, 3, 0), ("line", 3, 3, 0), ("last", 3, 0, 1),
    ("sum", 0, 0, 1), ("sum", 0, 0, 0), ("back", 1), ("last", 3, 2, 1), ("last", 3, 1, 1), ("hidden", 2),
    ("sum", 0, 1, 0), ("last", 3, 2, 0), ("sum", 0, 2, 1), ("sum", 0, 1, 1), ("last", 3, 3, 1),
    ("last", 3, 3, 0), ("last", 3, 1, 0), ("down", 2), ("sum", 1, 0, 1), ("sum", 1, 0, 0), ("hidden", 3),
    ("back", 2), ("sum", 1, 1, 1), ("sum", 0, 2, 0), ("down", 3), ("sum", 1, 2, 1), ("back", 3),
    ("sum", 1, 2, 0), ("sum", 1, 1, 0), ("sum", 2, 0, 1), ("sum", 2, 0, 0), ("sum", 3, 0, 1),
    ("sum", 3, 0, 0), ("sum", 2, 1, 1), ("sum", 3, 1, 1), ("sum", 2, 1, 0), ("sum", 3, 2, 1), ("home", 0, 1),
    ("home", 1, 1), ("sum", 3, 1, 0), ("sum", 2, 2, 1), ("sum", 3, 2, 0), ("drain_out", 0), ("drain_out", 1),
    ("drain_out", 2), ("drain_out", 3), ("home", 3, 1), ("sum", 2, 2, 0), ("home", 1, 0), ("final", 1),
    ("home", 0, 0), ("home", 2, 1), ("home", 3, 0), ("final", 0), ("drain_back", 0), ("drain_back", 1),
    ("drain_back", 2), ("final", 3), ("home", 2, 0), ("final", 2), ("drain_back", 3),
)


def ring_kernel(
    zs, tok_ref, gain_ref, ids_ref, score_ref, prob_ref, gate_hbm, up_hbm, down_hbm, out_ref,
    xg, stage, part, pair_in, last_in, line_in, first_in, fin_in, hid, scales, wgu, wd, w_sem,
    stage_send, stage_recv, gather_recv, own_send, first_send, line_send, last_send,
    mate_send, mate_recv, pair_send, pair_recv, back_send, back_recv, sum_send, sum_recv,
    home_send, home_recv, fin_send, fin_recv,
):
    me = lax.axis_index("ep")
    core = lax.rem(me, 2)
    x = lax.rem(lax.div(me, 2), 2)
    y = lax.rem(lax.div(me, 4), 2)
    z = lax.div(me, 8)
    other = 1 - core

    def device(zz, yy, xx, cc):
        return ((zz * 2 + yy) * 2 + xx) * 2 + cc

    partner = device(z, y, x, other)
    first_dev = device(z, y + core * (1 - 2 * y), x + other * (1 - 2 * x), core)
    last_dev = device(z, y + other * (1 - 2 * y), x + core * (1 - 2 * x), core)
    has = (z > 0, z < zs - 1)

    def column(fr, lr):
        dx = other * fr + core * lr
        dy = core * fr + other * lr
        xx = x + dx * (1 - 2 * x)
        yy = y + dy * (1 - 2 * y)
        return (xx * 2 + yy) * zs

    cols = [[column(fr, lr) for lr in (0, 1)] for fr in (0, 1)]
    near = [sorted(range(zs), key=lambda q, zz=zz: (abs(q - zz), -q if zz < zs // 2 else q))
            for zz in range(zs)]
    planes = []
    for i in range(zs):
        q = jnp.int32(near[0][i])
        for zz in range(1, zs):
            q = jnp.where(z == zz, near[zz][i], q)
        planes.append(q)
    below = [q < z for q in planes]
    away = [jnp.where(b, z + 1, z - 1) for b in below]
    away_ok = [jnp.logical_and(a >= 0, a < zs) for a in away]
    toward = [jnp.where(b, z - 1, z + 1) for b in below]
    side_of = [jnp.where(b, 1, 0) for b in below]

    model_width = tok_ref.shape[1]
    half = model_width // 2
    count = tok_ref.shape[0]
    rows = stage.shape[1]
    blocks = 4 * zs

    copies = [
        pltpu.make_async_copy(gate_hbm.at[0], wgu.at[:, : wgu.shape[1] // 2], w_sem.at[0]),
        pltpu.make_async_copy(up_hbm.at[0], wgu.at[:, wgu.shape[1] // 2 :], w_sem.at[1]),
        pltpu.make_async_copy(down_hbm.at[0, :, :half], wd.at[0], w_sem.at[2]),
        pltpu.make_async_copy(down_hbm.at[0, :, half:], wd.at[1], w_sem.at[3]),
    ]
    for copy in copies:
        copy.start()

    barrier = pltpu.get_barrier_semaphore()
    for peer in (partner, first_dev, last_dev):
        pl.semaphore_signal(barrier, inc=1, device_id=(peer,), device_id_type=MESH)
    for d in (0, 1):
        @pl.when(has[d])
        def _():
            pl.semaphore_signal(
                barrier, inc=1, device_id=(device(z - 1 + 2 * d, y, x, core),), device_id_type=MESH
            )

    def remote(src, dst, send_sem, recv_sem, target):
        return pltpu.make_async_remote_copy(
            src_ref=src, dst_ref=dst, send_sem=send_sem, recv_sem=recv_sem,
            device_id=(target,), device_id_type=MESH,
        )

    def landed(ref, sem):
        remote(ref, ref, sem, sem, partner).wait_recv()

    def sent(ref, sem):
        remote(ref, ref, sem, sem, partner).wait_send()

    def wide(k):
        return half + LANES if k == 0 else half

    def block(h, k, slot):
        return xg.at[h, k, slot, :, pl.ds(0, wide(k))]

    def span(h, k, n):
        return xg.at[h, k, pl.ds(0, n), :, pl.ds(0, wide(k))]

    own_slot = cols[0][0] + z

    values = tok_ref[...].astype(jnp.float32)
    average = jnp.sum(values, axis=1, keepdims=True) * (1.0 / model_width)
    centred = values - average
    variance = jnp.sum(centred * centred, axis=1, keepdims=True) * (1.0 / model_width)
    normed = (centred * lax.rsqrt(variance + eps_norm) * gain_ref[...]).astype(jnp.bfloat16)
    for c in (0, 1):
        @pl.when(core == c)
        def _():
            for j in range(CHUNKS // 2):
                piece = normed[j * rows : (j + 1) * rows]
                mine = piece[:, :half] if c == 0 else piece[:, half:]
                theirs = piece[:, half:] if c == 0 else piece[:, :half]
                xg[c, 2 * j + c, own_slot, :, :half] = mine
                stage[j] = theirs
    score = [score_ref[k : k + 1, :] for k in range(TOP_K)]
    top = functools.reduce(jnp.maximum, score)
    exps = [jnp.exp(s - top) for s in score]
    total = functools.reduce(jnp.add, exps)
    row = lax.broadcasted_iota(jnp.int32, (rows, count), 0)
    tags = jnp.zeros((rows, count), jnp.float32)
    for k in range(TOP_K):
        weight = exps[k] / total * prob_ref[...]
        high = weight.astype(jnp.bfloat16).astype(jnp.float32)
        tags = jnp.where(row == k, ids_ref[k : k + 1, :].astype(jnp.float32), tags)
        tags = jnp.where(row == TOP_K + k, high, tags)
        tags = jnp.where(row == 2 * TOP_K + k, weight - high, tags)
    tags = jnp.concatenate([tags, jnp.zeros((rows, LANES - count), jnp.float32)], axis=1)
    xg[core, 0, own_slot, :, half:] = tags.astype(jnp.bfloat16)

    inside = jnp.logical_and(has[0], has[1])

    @pl.when(inside)
    def _():
        pl.semaphore_wait(barrier, 5)

    @pl.when(jnp.logical_not(inside))
    def _():
        pl.semaphore_wait(barrier, 4)

    for j in range(CHUNKS // 2):
        k = 2 * j + core
        remote(stage.at[j], xg.at[core * 0 + other, k, own_slot, :, pl.ds(0, half)],
               stage_send.at[j], stage_recv.at[k], partner).start()

    def spread(k, slot, fr, i):
        ref = block(core, k, slot)
        sem = gather_recv.at[k, slot]
        if i == 0:
            for d in (0, 1):
                @pl.when(has[d])
                def _():
                    remote(ref, ref, own_send.at[k, d], sem, device(z - 1 + 2 * d, y, x, core)).start()
        else:
            @pl.when(away_ok[i])
            def _():
                remote(ref, ref, line_send.at[k, i], sem, device(away[i], y, x, core)).start()
        remote(ref, ref, last_send.at[k], sem, last_dev).start()
        remote(ref, ref, mate_send.at[k], mate_recv.at[k], partner).start()

    def own(k):
        @pl.when(core != k % 2)
        def _():
            landed(xg.at[core, k, own_slot, :, pl.ds(0, half)], stage_recv.at[k])
        ref = block(core, k, own_slot)
        remote(ref, ref, first_send.at[k], gather_recv.at[k, own_slot], first_dev).start()
        spread(k, own_slot, 0, 0)

    def first(k):
        slot = cols[1][0] + z
        landed(block(core, k, slot), gather_recv.at[k, slot])
        spread(k, slot, 1, 0)

    def line(k, i, fr):
        slot = cols[fr][0] + planes[i]
        landed(block(core, k, slot), gather_recv.at[k, slot])
        spread(k, slot, fr, i)

    def last(k, i, fr):
        slot = cols[fr][1] + planes[i]
        ref = block(core, k, slot)
        landed(ref, gather_recv.at[k, slot])
        remote(ref, ref, mate_send.at[k], mate_recv.at[k], partner).start()

    def hidden(k):
        landed(span(other, k, blocks), mate_recv.at[k])
        if k == 0:
            for copy in copies:
                copy.wait()
            expert = me.astype(jnp.float32)
            for h in (0, 1):
                tags = xg[h, 0, :, :, half:].astype(jnp.float32)
                scale = jnp.zeros((blocks, LANES), jnp.float32)
                for n in range(TOP_K):
                    value = tags[:, TOP_K + n, :] + tags[:, 2 * TOP_K + n, :]
                    scale += jnp.where(tags[:, n, :] == expert, value, 0.0)
                scales[h] = scale
        shape = (blocks, rows, LANES)
        pick = lax.broadcasted_iota(jnp.int32, shape, 2) == (
            lax.broadcasted_iota(jnp.int32, shape, 1) + rows * (k // 2))
        scale = jnp.sum(jnp.where(pick, scales[k % 2][:, None, :], 0.0), axis=2, keepdims=True)
        scale = scale.reshape(blocks * rows, 1)
        left = xg[0, k, :, :, :half].reshape(blocks * rows, half)
        right = xg[1, k, :, :, :half].reshape(blocks * rows, half)
        acts = jnp.dot(left, wgu[:half, :], preferred_element_type=jnp.float32) + jnp.dot(
            right, wgu[half:, :], preferred_element_type=jnp.float32
        )
        inner = hid.shape[1]
        hid[...] = (jax.nn.silu(acts[:, :inner]) * acts[:, inner:] * scale).astype(jnp.bfloat16)

    def down(k):
        step = half // 3 if half % (3 * LANES) == 0 else half
        for h in (other, core):
            for at in range(0, half, step):
                out = jnp.dot(hid[...], wd[h, :, at : at + step], preferred_element_type=jnp.float32)
                part[h, k, :, :, at : at + step] = out.astype(jnp.bfloat16).reshape(blocks, rows, step)
            if h is other:
                remote(part.at[other, k], pair_in.at[k], pair_send.at[k], pair_recv.at[k], partner).start()

    def back(k):
        landed(pair_in.at[k], pair_recv.at[k])
        for i in range(zs - 1, -1, -1):
            for fr in (0, 1):
                slot = cols[fr][1] + planes[i]
                part[core, k, slot] = part[core, k, slot] + pair_in[k, slot]
                remote(part.at[core, k, slot], last_in.at[k, fr, planes[i]], back_send.at[k],
                       back_recv.at[k, fr, planes[i]], last_dev).start()

    def gathered(k, fr, q):
        slot = cols[fr][0] + q
        landed(last_in.at[k, fr, q], back_recv.at[k, fr, q])
        held = part[core, k, slot].astype(jnp.float32) + pair_in[k, slot].astype(jnp.float32)
        part[core, k, slot] = (held + last_in[k, fr, q].astype(jnp.float32)).astype(jnp.bfloat16)
        return slot

    def line_sum(k, j, fr):
        i = zs - 1 - j
        q = planes[i]
        slot = gathered(k, fr, q)

        @pl.when(away_ok[i])
        def _():
            landed(line_in.at[k, side_of[i], fr, q], sum_recv.at[k, side_of[i], fr, q])
            part[core, k, slot] = part[core, k, slot] + line_in[k, side_of[i], fr, q]

        remote(part.at[core, k, slot], line_in.at[k, side_of[i], fr, q], sum_send.at[k],
               sum_recv.at[k, side_of[i], fr, q], device(toward[i], y, x, core)).start()

    def home(k, fr):
        slot = gathered(k, fr, z)
        for d in (0, 1):
            @pl.when(has[d])
            def _():
                landed(line_in.at[k, d, fr, z], sum_recv.at[k, d, fr, z])
                part[core, k, slot] = part[core, k, slot] + line_in[k, d, fr, z]
        if fr == 1:
            remote(part.at[core, k, slot], first_in.at[k], home_send.at[k], home_recv.at[k],
                   first_dev).start()

    def final(k):
        landed(first_in.at[k], home_recv.at[k])
        total = part[core, k, own_slot] + first_in[k]
        j = k // 2

        @pl.when(core == k % 2)
        def _():
            out_ref[j * rows : (j + 1) * rows, pl.ds(pl.multiple_of(core * half, LANES), half)] = total

        @pl.when(core != k % 2)
        def _():
            part[core, k, own_slot] = total
            remote(part.at[core, k, own_slot], fin_in.at[j], fin_send.at[j], fin_recv.at[j],
                   partner).start()

    def drain_out(k):
        @pl.when(core == k % 2)
        def _():
            sent(stage.at[k // 2], stage_send.at[k // 2])
        sent(block(core, k, own_slot), first_send.at[k])
        for d in (0, 1):
            @pl.when(has[d])
            def _():
                sent(span(core, k, 2), own_send.at[k, d])
        for i in range(1, zs):
            @pl.when(away_ok[i])
            def _():
                sent(span(core, k, 2), line_send.at[k, i])
        sent(span(core, k, 2 * zs), last_send.at[k])
        sent(span(core, k, blocks), mate_send.at[k])

    def drain_back(k):
        sent(part.at[other, k], pair_send.at[k])
        sent(part.at[core, k, pl.ds(0, 2 * zs)], back_send.at[k])
        sent(part.at[core, k, pl.ds(0, 2 * (zs - 1))], sum_send.at[k])
        sent(part.at[core, k, 0], home_send.at[k])

    steps = dict(own=own, first=first, line=line, last=last, hidden=hidden, down=down, back=back,
                 sum=line_sum, home=home, final=final, drain_out=drain_out, drain_back=drain_back)
    for name, *rest in ORDER:
        steps[name](*rest)

    for j in range(CHUNKS // 2):
        landed(fin_in.at[j], fin_recv.at[j])
        out_ref[j * rows : (j + 1) * rows, pl.ds(pl.multiple_of(other * half, LANES), half)] = fin_in[j]
    for j in range(CHUNKS // 2):
        sent(fin_in.at[j], fin_send.at[j])


def ring_local(
    zs, tokens, norm_gain, expert_ids, expert_scores, group_prob, gate_weight, up_weight, down_weight
):
    count, width = tokens.shape
    inner = gate_weight.shape[2]
    half = width // 2
    rows = 2 * count // CHUNKS
    blocks = 4 * zs
    kind = jnp.bfloat16
    vmem = pl.BlockSpec(memory_space=pltpu.VMEM)
    hbm = pl.BlockSpec(memory_space=pl.ANY)
    dma = pltpu.SemaphoreType.DMA
    c = CHUNKS
    scratch = [
        pltpu.VMEM((2, c, blocks, rows, half + LANES), kind),
        pltpu.VMEM((c // 2, rows, half), kind),
        pltpu.VMEM((2, c, blocks, rows, half), kind),
        pltpu.VMEM((c, blocks, rows, half), kind),
        pltpu.VMEM((c, 2, zs, rows, half), kind),
        pltpu.VMEM((c, 2, 2, zs, rows, half), kind),
        pltpu.VMEM((c, rows, half), kind),
        pltpu.VMEM((c // 2, rows, half), kind),
        pltpu.VMEM((blocks * rows, inner), kind),
        pltpu.VMEM((2, blocks, LANES), jnp.float32),
        pltpu.VMEM((width, 2 * inner), kind),
        pltpu.VMEM((2, inner, half), kind),
        dma((4,)),
        dma((c // 2,)), dma((c,)), dma((c, blocks)), dma((c, 2)), dma((c,)), dma((c, zs)), dma((c,)),
        dma((c,)), dma((c,)), dma((c,)), dma((c,)), dma((c,)), dma((c, 2, zs)),
        dma((c,)), dma((c, 2, 2, zs)),
        dma((c,)), dma((c,)), dma((c // 2,)), dma((c // 2,)),
    ]
    return pl.pallas_call(
        functools.partial(ring_kernel, zs),
        out_shape=jax.ShapeDtypeStruct((count, width), kind),
        in_specs=[vmem] * 5 + [hbm] * 3,
        out_specs=vmem,
        scratch_shapes=scratch,
        compiler_params=pltpu.CompilerParams(
            collective_id=0, has_side_effects=True, vmem_limit_bytes=60 * 1024 * 1024
        ),
    )(
        tokens, norm_gain[None, :], expert_ids.T, expert_scores.T, group_prob[None, :], gate_weight, up_weight, down_weight,
    )


def solution(mesh):
    in_specs = (
        P("ep", None),
        P(),
        P("ep", None),
        P("ep", None),
        P("ep"),
        P("ep", None, None),
        P("ep", None, None),
        P("ep", None, None),
    )
    out_specs = P("ep", None)
    devices = mesh.shape["ep"]
    body = functools.partial(ring_local, GROUPS) if devices == GROUPS * 8 else local
    return jax.shard_map(body, mesh=mesh, in_specs=in_specs, out_specs=out_specs, check_vma=False)
```

```python
import functools

import jax
import jax.numpy as jnp
from jax import lax
from jax.experimental import pallas as pl
from jax.experimental.pallas import tpu as pltpu
from jax.sharding import PartitionSpec as P

GROUPS = 4
TOP_K = 4
LANES = 128
MESH = pl.DeviceIdType.MESH


eps_norm = 1e-05


def layer_norm(tokens, norm_gain):
    values = tokens.astype(jnp.float32)
    average = jnp.mean(values, axis=1, keepdims=True)
    centred = values - average
    variance = jnp.mean(centred * centred, axis=1, keepdims=True)
    return (centred * lax.rsqrt(variance + eps_norm) * norm_gain[None, :]).astype(jnp.bfloat16)


def mixing_weights(expert_scores, group_prob):
    shifted = expert_scores - jnp.max(expert_scores, axis=1, keepdims=True)
    exp_scores = jnp.exp(shifted)
    return exp_scores / jnp.sum(exp_scores, axis=1, keepdims=True) * group_prob[:, None]


def expert_rows(flat_rows, gate_matrix, up_matrix, down_matrix):
    gate_act = jnp.dot(flat_rows, gate_matrix, preferred_element_type=jnp.float32)
    up_act = jnp.dot(flat_rows, up_matrix, preferred_element_type=jnp.float32)
    hidden = (jax.nn.silu(gate_act) * up_act).astype(jnp.bfloat16)
    return jnp.dot(hidden, down_matrix, preferred_element_type=jnp.float32).astype(jnp.bfloat16)


def local(
    tokens, norm_gain, expert_ids, expert_scores, group_prob, gate_weight, up_weight, down_weight
):
    normed = layer_norm(tokens, norm_gain)
    weights_tok = mixing_weights(expert_scores, group_prob)
    tok_count = tokens.shape[0]
    model_width = tokens.shape[1]
    expert_count = lax.axis_size("ep")
    group_size = expert_count // GROUPS
    capacity = (tok_count * TOP_K + group_size - 1) // group_size
    expert_iota = jnp.arange(expert_count, dtype=jnp.int32)
    slot_iota = jnp.arange(capacity, dtype=jnp.int32)
    matches = expert_ids[:, :, None] == expert_iota[None, None, :]
    route_weight = jnp.sum(jnp.where(matches, weights_tok[:, :, None], 0.0), axis=1)
    gate_matrix = gate_weight[0]
    up_matrix = up_weight[0]
    down_matrix = down_weight[0]
    chosen = jnp.sum(matches.astype(jnp.int32), axis=1)
    order_rank = jnp.cumsum(chosen, axis=0) - chosen
    slot_map = (chosen.T[:, None, :] == 1) & (order_rank.T[:, None, :] == slot_iota[None, :, None])
    outgoing = jnp.einsum(
        "emt,td->emd", slot_map.astype(jnp.bfloat16), normed, preferred_element_type=jnp.float32
    ).astype(jnp.bfloat16)
    received = lax.all_to_all(outgoing, "ep", split_axis=0, concat_axis=0, tiled=True)
    flat_rows = received.reshape(-1, model_width)
    results = expert_rows(flat_rows, gate_matrix, up_matrix, down_matrix).reshape(received.shape)
    returned_rows = lax.all_to_all(results, "ep", split_axis=0, concat_axis=0, tiled=True)
    slot_scale = jnp.where(slot_map, route_weight.T[:, None, :], 0.0)
    mixture = jnp.einsum(
        "emt,emd->td",
        slot_scale,
        returned_rows.astype(jnp.float32),
        precision=lax.Precision.HIGHEST,
    )
    return mixture.astype(jnp.bfloat16)

CHUNKS = 4


END_ORDER = (
    ("own", 0), ("own", 2), ("own", 1), ("firstq", 0, 0), ("own", 3), ("line", 0, 1, 0), ("line", 2, 1, 0),
    ("line", 1, 1, 0), ("first", 1), ("line", 0, 2, 0), ("line", 3, 1, 0), ("first", 2), ("last", 1, 0, 0),
    ("line", 3, 2, 0), ("last", 1, 1, 0), ("firstq", 0, 1), ("firstq", 0, 2), ("line", 0, 3, 0),
    ("last", 0, 2, 0), ("last", 2, 1, 0), ("firstq", 0, 3), ("line", 2, 1, 1), ("line", 3, 3, 0),
    ("last", 0, 1, 1), ("firstq", 3, 1), ("last", 0, 1, 0), ("last", 0, 0, 1), ("line", 2, 2, 0),
    ("last", 2, 0, 0), ("firstq", 3, 2), ("last", 3, 0, 0), ("last", 0, 0, 0), ("line", 2, 3, 1),
    ("line", 1, 2, 0), ("last", 0, 2, 1), ("last", 0, 3, 0), ("last", 0, 3, 1), ("line", 2, 3, 0),
    ("line", 2, 2, 1), ("firstq", 3, 3), ("hidden", 0), ("line", 1, 3, 1), ("last", 3, 2, 1),
    ("last", 2, 2, 0), ("firstq", 3, 0), ("last", 3, 3, 0), ("last", 2, 0, 1), ("last", 2, 1, 1),
    ("down", 0, 0), ("line", 1, 2, 1), ("last", 2, 3, 0), ("last", 2, 3, 1), ("last", 2, 2, 1),
    ("last", 3, 2, 0), ("line", 1, 3, 0), ("last", 3, 1, 1), ("last", 3, 1, 0), ("line", 1, 1, 1),
    ("down", 0, 1), ("last", 3, 3, 1), ("back", 0), ("hidden", 2), ("last", 3, 0, 1), ("last", 1, 0, 1),
    ("last", 1, 2, 0), ("down", 2, 0), ("down", 2, 1), ("last", 1, 3, 0), ("fsum", 0, 0), ("last", 1, 1, 1),
    ("hidden", 3), ("last", 1, 3, 1), ("last", 1, 2, 1), ("back", 2), ("down", 3, 0), ("zsum", 0, 0),
    ("hidden", 1), ("down", 3, 1), ("fsum", 0, 1), ("back", 3), ("sum", 2, 0, 1), ("sum", 2, 1, 1),
    ("down", 1, 0), ("zsum", 0, 1), ("sum", 2, 2, 1), ("fsum", 3, 0), ("sum", 2, 1, 0), ("sum", 2, 0, 0),
    ("down", 1, 1), ("back", 1), ("zsum", 3, 0), ("sum", 1, 0, 1), ("sum", 1, 1, 1), ("fsum", 3, 1),
    ("fsum", 3, 2), ("fsum", 0, 2), ("fsum", 3, 3), ("sum", 1, 0, 0), ("sum", 1, 2, 1), ("sum", 1, 1, 0),
    ("zsum", 3, 1), ("sum", 2, 2, 0), ("home", 2, 1), ("sum", 1, 2, 0), ("zsum", 3, 2), ("zsum", 0, 2),
    ("fsum", 0, 3), ("home", 1, 1), ("home", 2, 0), ("final", 2), ("homez", 3), ("homez", 0), ("home", 1, 0),
    ("drain_out", 0), ("drain_out", 1), ("drain_out", 2), ("drain_out", 3), ("drain_back", 0),
    ("drain_back", 2), ("drain_back", 3), ("final", 1), ("drain_back", 1),
)

INNER_ORDER = (
    ("own", 2), ("own", 0), ("own", 1), ("own", 3), ("line", 0, 2, 0), ("line", 0, 1, 0), ("line", 2, 2, 0),
    ("first", 2), ("firstq", 3, 0), ("line", 3, 1, 0), ("line", 0, 3, 0), ("line", 2, 1, 0),
    ("line", 3, 2, 0), ("first", 1), ("firstq", 0, 0), ("line", 1, 2, 1), ("line", 3, 3, 0),
    ("line", 2, 2, 1), ("last", 0, 2, 0), ("firstq", 0, 1), ("firstq", 3, 1), ("firstq", 0, 3),
    ("firstq", 0, 2), ("last", 2, 0, 0), ("line", 1, 2, 0), ("last", 0, 0, 0), ("line", 1, 1, 0),
    ("line", 1, 3, 1), ("firstq", 3, 2), ("line", 2, 3, 1), ("last", 3, 1, 0), ("line", 2, 3, 0),
    ("last", 0, 1, 0), ("last", 3, 2, 0), ("firstq", 3, 3), ("line", 2, 1, 1), ("last", 0, 1, 1),
    ("last", 3, 0, 1), ("last", 0, 3, 0), ("line", 1, 3, 0), ("last", 1, 2, 1), ("last", 0, 0, 1),
    ("last", 2, 0, 1), ("last", 0, 3, 1), ("line", 1, 1, 1), ("last", 2, 2, 1), ("last", 2, 2, 0),
    ("last", 0, 2, 1), ("last", 1, 2, 0), ("hidden", 0), ("last", 1, 3, 1), ("last", 3, 1, 1), ("down", 0, 0),
    ("down", 0, 1), ("last", 2, 1, 0), ("last", 3, 2, 1), ("last", 3, 3, 0), ("last", 3, 3, 1),
    ("last", 3, 0, 0), ("back", 0), ("last", 2, 1, 1), ("last", 1, 0, 0), ("last", 2, 3, 0), ("hidden", 3),
    ("down", 3, 0), ("down", 3, 1), ("last", 1, 3, 0), ("last", 2, 3, 1), ("last", 1, 1, 0), ("fsum", 0, 0),
    ("back", 3), ("hidden", 2), ("last", 1, 0, 1), ("last", 1, 1, 1), ("fsum", 0, 2), ("down", 2, 0),
    ("fsum", 3, 0), ("zsum", 0, 0), ("down", 2, 1), ("back", 2), ("hidden", 1), ("down", 1, 0),
    ("zsum", 0, 2), ("sum", 2, 0, 1), ("fsum", 3, 1), ("down", 1, 1), ("back", 1), ("sum", 2, 0, 0),
    ("sum", 2, 2, 1), ("zsum", 3, 0), ("sum", 1, 0, 1), ("sum", 2, 1, 1), ("fsum", 3, 3), ("sum", 2, 1, 0),
    ("sum", 1, 2, 1), ("fsum", 3, 2), ("fsum", 0, 1), ("fsum", 0, 3), ("zsum", 3, 1), ("sum", 1, 0, 0),
    ("sum", 1, 1, 1), ("sum", 2, 2, 0), ("home", 2, 1), ("zsum", 0, 1), ("sum", 1, 2, 0), ("zsum", 3, 2),
    ("home", 1, 1), ("sum", 1, 1, 0), ("home", 2, 0), ("home", 1, 0), ("final", 1), ("homez", 3),
    ("final", 2), ("drain_out", 0), ("drain_out", 1), ("drain_out", 2), ("drain_out", 3), ("drain_back", 1),
    ("drain_back", 2), ("drain_back", 3), ("homez", 0), ("drain_back", 0),
)

Z_FIRST = (True, False, False, True)


def ring_kernel(
    zs, tok_ref, gain_ref, ids_ref, score_ref, prob_ref, gate_hbm, up_hbm, down_hbm, out_ref,
    xg, stage, part, pair_in, last_in, line_in, first_in, fin_in, hid, scales, wgu, wd, w_sem,
    stage_send, stage_recv, gather_recv, own_send, first_send, line_send, last_send,
    mate_send, mate_recv, pair_send, pair_recv, back_send, back_recv, sum_send, sum_recv,
    home_send, home_recv, fin_send, fin_recv,
):
    me = lax.axis_index("ep")
    core = lax.rem(me, 2)
    x = lax.rem(lax.div(me, 2), 2)
    y = lax.rem(lax.div(me, 4), 2)
    z = lax.div(me, 8)
    other = 1 - core

    def device(zz, yy, xx, cc):
        return ((zz * 2 + yy) * 2 + xx) * 2 + cc

    partner = device(z, y, x, other)
    first_dev = device(z, y + core * (1 - 2 * y), x + other * (1 - 2 * x), core)
    last_dev = device(z, y + other * (1 - 2 * y), x + core * (1 - 2 * x), core)
    has = (z > 0, z < zs - 1)

    def column(fr, lr):
        dx = other * fr + core * lr
        dy = core * fr + other * lr
        xx = x + dx * (1 - 2 * x)
        yy = y + dy * (1 - 2 * y)
        return (xx * 2 + yy) * zs

    cols = [[column(fr, lr) for lr in (0, 1)] for fr in (0, 1)]
    near = [sorted(range(zs), key=lambda q, zz=zz: (abs(q - zz), -q if zz < zs // 2 else q))
            for zz in range(zs)]
    planes = []
    for i in range(zs):
        q = jnp.int32(near[0][i])
        for zz in range(1, zs):
            q = jnp.where(z == zz, near[zz][i], q)
        planes.append(q)
    below = [q < z for q in planes]
    away = [jnp.where(b, z + 1, z - 1) for b in below]
    toward = [jnp.where(b, z - 1, z + 1) for b in below]
    side_of = [jnp.where(b, 1, 0) for b in below]

    model_width = tok_ref.shape[1]
    half = model_width // 2
    count = tok_ref.shape[0]
    rows = stage.shape[1]
    blocks = 4 * zs
    inner = hid.shape[2]

    copies = [
        pltpu.make_async_copy(gate_hbm.at[0], wgu.at[:, : wgu.shape[1] // 2], w_sem.at[0]),
        pltpu.make_async_copy(up_hbm.at[0], wgu.at[:, wgu.shape[1] // 2 :], w_sem.at[1]),
        pltpu.make_async_copy(down_hbm.at[0, :, :half], wd.at[0], w_sem.at[2]),
        pltpu.make_async_copy(down_hbm.at[0, :, half:], wd.at[1], w_sem.at[3]),
    ]
    for copy in copies:
        copy.start()

    barrier = pltpu.get_barrier_semaphore()
    for peer in (partner, first_dev, last_dev):
        pl.semaphore_signal(barrier, inc=1, device_id=(peer,), device_id_type=MESH)
    for d in (0, 1):
        @pl.when(has[d])
        def _():
            pl.semaphore_signal(
                barrier, inc=1, device_id=(device(z - 1 + 2 * d, y, x, core),), device_id_type=MESH
            )

    def remote(src, dst, send_sem, recv_sem, target):
        return pltpu.make_async_remote_copy(
            src_ref=src, dst_ref=dst, send_sem=send_sem, recv_sem=recv_sem,
            device_id=(target,), device_id_type=MESH,
        )

    def landed(ref, sem):
        remote(ref, ref, sem, sem, partner).wait_recv()

    def sent(ref, sem):
        remote(ref, ref, sem, sem, partner).wait_send()

    def wide(k):
        return half + LANES if k == 0 else half

    def block(h, k, slot):
        return xg.at[h, k, slot, :, pl.ds(0, wide(k))]

    def span(h, k, n):
        return xg.at[h, k, pl.ds(0, n), :, pl.ds(0, wide(k))]

    own_slot = cols[0][0] + z

    values = tok_ref[...].astype(jnp.float32)
    average = jnp.sum(values, axis=1, keepdims=True) * (1.0 / model_width)
    centred = values - average
    variance = jnp.sum(centred * centred, axis=1, keepdims=True) * (1.0 / model_width)
    normed = (centred * lax.rsqrt(variance + eps_norm) * gain_ref[...]).astype(jnp.bfloat16)
    for c in (0, 1):
        @pl.when(core == c)
        def _():
            for j in range(CHUNKS // 2):
                piece = normed[j * rows : (j + 1) * rows]
                mine = piece[:, :half] if c == 0 else piece[:, half:]
                theirs = piece[:, half:] if c == 0 else piece[:, :half]
                xg[c, 2 * j + c, own_slot, :, :half] = mine
                stage[j] = theirs
    score = [score_ref[k : k + 1, :] for k in range(TOP_K)]
    top = functools.reduce(jnp.maximum, score)
    exps = [jnp.exp(s - top) for s in score]
    total = functools.reduce(jnp.add, exps)
    row = lax.broadcasted_iota(jnp.int32, (rows, count), 0)
    tags = jnp.zeros((rows, count), jnp.float32)
    for k in range(TOP_K):
        weight = exps[k] / total * prob_ref[...]
        high = weight.astype(jnp.bfloat16).astype(jnp.float32)
        tags = jnp.where(row == k, ids_ref[k : k + 1, :].astype(jnp.float32), tags)
        tags = jnp.where(row == TOP_K + k, high, tags)
        tags = jnp.where(row == 2 * TOP_K + k, weight - high, tags)
    tags = jnp.concatenate([tags, jnp.zeros((rows, LANES - count), jnp.float32)], axis=1)
    xg[core, 0, own_slot, :, half:] = tags.astype(jnp.bfloat16)

    inside = jnp.logical_and(has[0], has[1])

    @pl.when(inside)
    def _():
        pl.semaphore_wait(barrier, 5)

    @pl.when(jnp.logical_not(inside))
    def _():
        pl.semaphore_wait(barrier, 4)

    for j in range(CHUNKS // 2):
        k = 2 * j + core
        remote(stage.at[j], xg.at[core * 0 + other, k, own_slot, :, pl.ds(0, half)],
               stage_send.at[j], stage_recv.at[k], partner).start()

    onward = jnp.where(z == 0, 1, z - 1)

    def program(at_end, order):
        sides = (jnp.where(z == 0, 1, 0),) if at_end else (0, 1)

        def out_z(ref, k, slot, sem_of):
            for n, d in enumerate((onward,) if at_end else (z - 1, z + 1)):
                remote(ref, ref, sem_of(n), gather_recv.at[k, slot], device(d, y, x, core)).start()

        def spread(k, fr, i):
            slot = cols[fr][0] + planes[i]
            ref = block(core, k, slot)
            sem = gather_recv.at[k, slot]
            if i == 0:
                out_z(ref, k, slot, lambda n: own_send.at[k, n])
            elif not at_end:
                remote(ref, ref, line_send.at[k, i], sem, device(away[i], y, x, core)).start()
            if Z_FIRST[k] and fr == 0:
                remote(ref, ref, first_send.at[k], sem, first_dev).start()
            remote(ref, ref, last_send.at[k], sem, last_dev).start()
            remote(ref, ref, mate_send.at[k], mate_recv.at[k], partner).start()

        def own(k):
            @pl.when(core != k % 2)
            def _():
                landed(xg.at[core, k, own_slot, :, pl.ds(0, half)], stage_recv.at[k])
            if not Z_FIRST[k]:
                ref = block(core, k, own_slot)
                remote(ref, ref, first_send.at[k], gather_recv.at[k, own_slot], first_dev).start()
            spread(k, 0, 0)

        def arrived(k, fr, lr, i):
            slot = cols[fr][lr] + planes[i]
            ref = block(core, k, slot)
            landed(ref, gather_recv.at[k, slot])
            return ref, slot

        def first(k):
            arrived(k, 1, 0, 0)
            spread(k, 1, 0)

        def line(k, i, fr):
            arrived(k, fr, 0, i)
            spread(k, fr, i)

        def firstq(k, i):
            ref, slot = arrived(k, 1, 0, i)
            remote(ref, ref, last_send.at[k], gather_recv.at[k, slot], last_dev).start()
            remote(ref, ref, mate_send.at[k], mate_recv.at[k], partner).start()

        def last(k, i, fr):
            ref, slot = arrived(k, fr, 1, i)
            remote(ref, ref, mate_send.at[k], mate_recv.at[k], partner).start()

        def hidden(k):
            landed(span(other, k, blocks), mate_recv.at[k])
            if order[[o[0] for o in order].index("hidden")][1] == k:
                start_compute()
            shape = (blocks, rows, LANES)
            pick = lax.broadcasted_iota(jnp.int32, shape, 2) == (
                lax.broadcasted_iota(jnp.int32, shape, 1) + rows * (k // 2))
            scale = jnp.sum(jnp.where(pick, scales[k % 2][:, None, :], 0.0), axis=2, keepdims=True)
            scale = scale.reshape(blocks * rows, 1)
            left = xg[0, k, :, :, :half].reshape(blocks * rows, half)
            right = xg[1, k, :, :, :half].reshape(blocks * rows, half)
            acts = jnp.dot(left, wgu[:half, :], preferred_element_type=jnp.float32) + jnp.dot(
                right, wgu[half:, :], preferred_element_type=jnp.float32
            )
            value = jax.nn.silu(acts[:, :inner]) * acts[:, inner:] * scale
            hid[k] = value.astype(jnp.bfloat16)

        def start_compute():
            for copy in copies:
                copy.wait()
            expert = me.astype(jnp.float32)
            for h in (0, 1):
                tags = xg[h, 0, :, :, half:].astype(jnp.float32)
                scale = jnp.zeros((blocks, LANES), jnp.float32)
                for n in range(TOP_K):
                    value = tags[:, TOP_K + n, :] + tags[:, 2 * TOP_K + n, :]
                    scale += jnp.where(tags[:, n, :] == expert, value, 0.0)
                scales[h] = scale

        def down(k, i):
            step = half // 3 if half % (3 * LANES) == 0 else half
            h = core if i else other
            for at in range(0, half, step):
                out = jnp.dot(hid[k], wd[h, :, at : at + step], preferred_element_type=jnp.float32)
                part[h, k, :, :, at : at + step] = out.astype(jnp.bfloat16).reshape(blocks, rows, step)
            if i == 0:
                remote(part.at[other, k], pair_in.at[k], pair_send.at[k], pair_recv.at[k], partner).start()

        def back(k):
            landed(pair_in.at[k], pair_recv.at[k])
            for i in range(zs - 1, -1, -1):
                for fr in (0, 1):
                    slot = cols[fr][1] + planes[i]
                    part[core, k, slot] = part[core, k, slot] + pair_in[k, slot]
                    remote(part.at[core, k, slot], last_in.at[k, fr, planes[i]], back_send.at[k],
                           back_recv.at[k, fr, planes[i]], last_dev).start()

        def collect(k, fr, q, from_line=(), from_first=False):
            slot = cols[fr][0] + q
            landed(last_in.at[k, fr, q], back_recv.at[k, fr, q])
            held = part[core, k, slot].astype(jnp.float32) + pair_in[k, slot].astype(jnp.float32)
            held = held + last_in[k, fr, q].astype(jnp.float32)
            if from_first:
                landed(first_in.at[k, q], home_recv.at[k, q])
                held = held + first_in[k, q].astype(jnp.float32)
            for side in from_line:
                landed(line_in.at[k, side, fr, q], sum_recv.at[k, side, fr, q])
                held = held + line_in[k, side, fr, q].astype(jnp.float32)
            part[core, k, slot] = held.astype(jnp.bfloat16)
            return slot

        def line_sum(k, j, fr):
            i = zs - 1 - j
            q = planes[i]
            slot = collect(k, fr, q, () if at_end else (side_of[i],), Z_FIRST[k])
            remote(part.at[core, k, slot], line_in.at[k, side_of[i], fr, q], sum_send.at[k],
                   sum_recv.at[k, side_of[i], fr, q], device(toward[i], y, x, core)).start()

        def zsum(k, j):
            line_sum(k, j, 0)

        def to_first(k, slot, q):
            remote(part.at[core, k, slot], first_in.at[k, q], home_send.at[k], home_recv.at[k, q],
                   first_dev).start()

        def fsum(k, j):
            q = planes[zs - 1 - j]
            to_first(k, collect(k, 1, q), q)

        def home(k, fr):
            slot = collect(k, fr, z, sides)
            if fr == 1:
                to_first(k, slot, z)

        def finish(k, total):
            j = k // 2

            @pl.when(core == k % 2)
            def _():
                out_ref[j * rows : (j + 1) * rows, pl.ds(pl.multiple_of(core * half, LANES), half)] = total

            @pl.when(core != k % 2)
            def _():
                remote(part.at[core, k, own_slot], fin_in.at[j], fin_send.at[j], fin_recv.at[j],
                       partner).start()

        def final(k):
            landed(first_in.at[k, z], home_recv.at[k, z])
            total = part[core, k, own_slot] + first_in[k, z]
            part[core, k, own_slot] = total
            finish(k, total)

        def homez(k):
            collect(k, 0, z, sides, True)
            finish(k, part[core, k, own_slot])

        def drain_out(k):
            @pl.when(core == k % 2)
            def _():
                sent(stage.at[k // 2], stage_send.at[k // 2])
            wide_z = 1 if Z_FIRST[k] else 2
            sent(span(core, k, zs if Z_FIRST[k] else 1), first_send.at[k])
            for n in (0,) if at_end else (0, 1):
                sent(span(core, k, wide_z), own_send.at[k, n])
            for i in () if at_end else range(1, zs):
                sent(span(core, k, wide_z), line_send.at[k, i])
            sent(span(core, k, 2 * zs), last_send.at[k])
            sent(span(core, k, blocks), mate_send.at[k])

        def drain_back(k):
            sent(part.at[other, k], pair_send.at[k])
            sent(part.at[core, k, pl.ds(0, 2 * zs)], back_send.at[k])
            sent(part.at[core, k, pl.ds(0, (1 if Z_FIRST[k] else 2) * (zs - 1))], sum_send.at[k])
            sent(part.at[core, k, pl.ds(0, zs if Z_FIRST[k] else 1)], home_send.at[k])

        steps = dict(own=own, first=first, line=line, firstq=firstq, last=last, hidden=hidden, down=down,
                     back=back, sum=line_sum, zsum=zsum, fsum=fsum, home=home, homez=homez, final=final,
                     drain_out=drain_out, drain_back=drain_back)
        for name, *rest in order:
            steps[name](*rest)

    pl.when(inside)(lambda: program(False, INNER_ORDER))
    pl.when(jnp.logical_not(inside))(lambda: program(True, END_ORDER))

    for j in range(CHUNKS // 2):
        landed(fin_in.at[j], fin_recv.at[j])
        out_ref[j * rows : (j + 1) * rows, pl.ds(pl.multiple_of(other * half, LANES), half)] = fin_in[j]
    for j in range(CHUNKS // 2):
        sent(fin_in.at[j], fin_send.at[j])


def ring_local(
    zs, tokens, norm_gain, expert_ids, expert_scores, group_prob, gate_weight, up_weight, down_weight
):
    count, width = tokens.shape
    inner = gate_weight.shape[2]
    half = width // 2
    rows = 2 * count // CHUNKS
    blocks = 4 * zs
    kind = jnp.bfloat16
    vmem = pl.BlockSpec(memory_space=pltpu.VMEM)
    hbm = pl.BlockSpec(memory_space=pl.ANY)
    dma = pltpu.SemaphoreType.DMA
    c = CHUNKS
    scratch = [
        pltpu.VMEM((2, c, blocks, rows, half + LANES), kind),
        pltpu.VMEM((c // 2, rows, half), kind),
        pltpu.VMEM((2, c, blocks, rows, half), kind),
        pltpu.VMEM((c, blocks, rows, half), kind),
        pltpu.VMEM((c, 2, zs, rows, half), kind),
        pltpu.VMEM((c, 2, 2, zs, rows, half), kind),
        pltpu.VMEM((c, zs, rows, half), kind),
        pltpu.VMEM((c // 2, rows, half), kind),
        pltpu.VMEM((c, blocks * rows, inner), kind),
        pltpu.VMEM((2, blocks, LANES), jnp.float32),
        pltpu.VMEM((width, 2 * inner), kind),
        pltpu.VMEM((2, inner, half), kind),
        dma((4,)),
        dma((c // 2,)), dma((c,)), dma((c, blocks)), dma((c, 2)), dma((c,)), dma((c, zs)), dma((c,)),
        dma((c,)), dma((c,)), dma((c,)), dma((c,)), dma((c,)), dma((c, 2, zs)),
        dma((c,)), dma((c, 2, 2, zs)),
        dma((c,)), dma((c, zs)), dma((c // 2,)), dma((c // 2,)),
    ]
    return pl.pallas_call(
        functools.partial(ring_kernel, zs),
        out_shape=jax.ShapeDtypeStruct((count, width), kind),
        in_specs=[vmem] * 5 + [hbm] * 3,
        out_specs=vmem,
        scratch_shapes=scratch,
        compiler_params=pltpu.CompilerParams(
            collective_id=0, has_side_effects=True, vmem_limit_bytes=60 * 1024 * 1024
        ),
    )(
        tokens, norm_gain[None, :], expert_ids.T, expert_scores.T, group_prob[None, :], gate_weight, up_weight, down_weight,
    )


def solution(mesh):
    in_specs = (
        P("ep", None),
        P(),
        P("ep", None),
        P("ep", None),
        P("ep"),
        P("ep", None, None),
        P("ep", None, None),
        P("ep", None, None),
    )
    out_specs = P("ep", None)
    devices = mesh.shape["ep"]
    body = functools.partial(ring_local, GROUPS) if devices == GROUPS * 8 else local
    return jax.shard_map(body, mesh=mesh, in_specs=in_specs, out_specs=out_specs, check_vma=False)
```

```python
import functools

import jax
import jax.numpy as jnp
from jax import lax
from jax.experimental import pallas as pl
from jax.experimental.pallas import tpu as pltpu
from jax.sharding import PartitionSpec as P

GROUPS = 4
TOP_K = 4
LANES = 128
MESH = pl.DeviceIdType.MESH


eps_norm = 1e-05


def layer_norm(tokens, norm_gain):
    values = tokens.astype(jnp.float32)
    average = jnp.mean(values, axis=1, keepdims=True)
    centred = values - average
    variance = jnp.mean(centred * centred, axis=1, keepdims=True)
    return (centred * lax.rsqrt(variance + eps_norm) * norm_gain[None, :]).astype(jnp.bfloat16)


def mixing_weights(expert_scores, group_prob):
    shifted = expert_scores - jnp.max(expert_scores, axis=1, keepdims=True)
    exp_scores = jnp.exp(shifted)
    return exp_scores / jnp.sum(exp_scores, axis=1, keepdims=True) * group_prob[:, None]


def expert_rows(flat_rows, gate_matrix, up_matrix, down_matrix):
    gate_act = jnp.dot(flat_rows, gate_matrix, preferred_element_type=jnp.float32)
    up_act = jnp.dot(flat_rows, up_matrix, preferred_element_type=jnp.float32)
    hidden = (jax.nn.silu(gate_act) * up_act).astype(jnp.bfloat16)
    return jnp.dot(hidden, down_matrix, preferred_element_type=jnp.float32).astype(jnp.bfloat16)


def local(
    tokens, norm_gain, expert_ids, expert_scores, group_prob, gate_weight, up_weight, down_weight
):
    normed = layer_norm(tokens, norm_gain)
    weights_tok = mixing_weights(expert_scores, group_prob)
    tok_count = tokens.shape[0]
    model_width = tokens.shape[1]
    expert_count = lax.axis_size("ep")
    group_size = expert_count // GROUPS
    capacity = (tok_count * TOP_K + group_size - 1) // group_size
    expert_iota = jnp.arange(expert_count, dtype=jnp.int32)
    slot_iota = jnp.arange(capacity, dtype=jnp.int32)
    matches = expert_ids[:, :, None] == expert_iota[None, None, :]
    route_weight = jnp.sum(jnp.where(matches, weights_tok[:, :, None], 0.0), axis=1)
    gate_matrix = gate_weight[0]
    up_matrix = up_weight[0]
    down_matrix = down_weight[0]
    chosen = jnp.sum(matches.astype(jnp.int32), axis=1)
    order_rank = jnp.cumsum(chosen, axis=0) - chosen
    slot_map = (chosen.T[:, None, :] == 1) & (order_rank.T[:, None, :] == slot_iota[None, :, None])
    outgoing = jnp.einsum(
        "emt,td->emd", slot_map.astype(jnp.bfloat16), normed, preferred_element_type=jnp.float32
    ).astype(jnp.bfloat16)
    received = lax.all_to_all(outgoing, "ep", split_axis=0, concat_axis=0, tiled=True)
    flat_rows = received.reshape(-1, model_width)
    results = expert_rows(flat_rows, gate_matrix, up_matrix, down_matrix).reshape(received.shape)
    returned_rows = lax.all_to_all(results, "ep", split_axis=0, concat_axis=0, tiled=True)
    slot_scale = jnp.where(slot_map, route_weight.T[:, None, :], 0.0)
    mixture = jnp.einsum(
        "emt,emd->td",
        slot_scale,
        returned_rows.astype(jnp.float32),
        precision=lax.Precision.HIGHEST,
    )
    return mixture.astype(jnp.bfloat16)

CHUNKS = 4


END_ORDER = (
    ("own", 0), ("own", 3), ("own", 2), ("firstq", 0, 0), ("own", 1), ("first", 3), ("line", 2, 1, 0),
    ("line", 0, 1, 0), ("line", 3, 1, 0), ("firstq", 2, 1), ("line", 0, 2, 0), ("line", 0, 3, 0),
    ("line", 1, 1, 1), ("last", 0, 0, 0), ("firstq", 0, 2), ("last", 0, 1, 0), ("firstq", 0, 1), ("first", 1),
    ("last", 2, 1, 1), ("last", 0, 2, 0), ("firstq", 0, 3), ("last", 0, 3, 0), ("line", 3, 2, 0),
    ("last", 3, 1, 0), ("line", 3, 1, 1), ("line", 3, 3, 1), ("last", 1, 1, 1), ("line", 3, 3, 0),
    ("last", 0, 1, 1), ("last", 0, 2, 1), ("line", 3, 2, 1), ("last", 0, 0, 1), ("last", 0, 3, 1),
    ("last", 2, 1, 0), ("last", 2, 0, 0), ("line", 1, 1, 0), ("last", 3, 0, 1), ("line", 2, 3, 0),
    ("line", 2, 2, 0), ("firstq", 2, 0), ("hidden", 0), ("last", 3, 1, 1), ("line", 1, 2, 0),
    ("last", 3, 2, 1), ("last", 3, 3, 0), ("last", 3, 0, 0), ("last", 1, 0, 1), ("last", 3, 3, 1),
    ("last", 3, 2, 0), ("down", 0, 0), ("line", 1, 2, 1), ("line", 1, 3, 0), ("last", 2, 3, 0),
    ("line", 1, 3, 1), ("firstq", 2, 2), ("last", 2, 2, 0), ("firstq", 2, 3), ("down", 0, 1),
    ("last", 1, 1, 0), ("back", 0), ("last", 2, 0, 1), ("last", 1, 0, 0), ("hidden", 3), ("last", 1, 2, 1),
    ("last", 1, 3, 0), ("last", 1, 2, 0), ("last", 1, 3, 1), ("down", 3, 0), ("hidden", 1), ("fsum", 0, 0),
    ("down", 3, 1), ("back", 3), ("down", 1, 0), ("last", 2, 3, 1), ("last", 2, 2, 1), ("zsum", 0, 0),
    ("down", 1, 1), ("back", 1), ("sum", 3, 0, 0), ("sum", 3, 0, 1), ("sum", 3, 1, 0), ("hidden", 2),
    ("down", 2, 0), ("sum", 3, 2, 1), ("sum", 3, 1, 1), ("down", 2, 1), ("back", 2), ("sum", 1, 0, 1),
    ("sum", 1, 0, 0), ("sum", 1, 1, 1), ("sum", 1, 2, 1), ("sum", 3, 2, 0), ("fsum", 2, 0), ("fsum", 2, 1),
    ("sum", 1, 1, 0), ("fsum", 0, 1), ("zsum", 2, 0), ("fsum", 2, 3), ("zsum", 2, 1), ("home", 3, 1),
    ("fsum", 2, 2), ("zsum", 0, 1), ("sum", 1, 2, 0), ("fsum", 0, 2), ("home", 1, 1), ("home", 3, 0),
    ("zsum", 2, 2), ("final", 3), ("home", 1, 0), ("fsum", 0, 3), ("zsum", 0, 2), ("final", 1), ("homez", 0),
    ("drain_out", 0), ("drain_out", 1), ("drain_out", 2), ("drain_out", 3), ("drain_back", 0),
    ("drain_back", 1), ("drain_back", 3), ("homez", 2), ("drain_back", 2),
)

INNER_ORDER = (
    ("own", 0), ("own", 2), ("own", 1), ("own", 3), ("line", 0, 2, 0), ("line", 0, 1, 0), ("line", 2, 1, 0),
    ("line", 3, 2, 0), ("first", 1), ("line", 0, 3, 0), ("firstq", 0, 0), ("firstq", 0, 2), ("line", 3, 3, 0),
    ("firstq", 0, 1), ("line", 3, 2, 1), ("first", 3), ("firstq", 0, 3), ("line", 3, 1, 0), ("last", 0, 2, 0),
    ("line", 3, 3, 1), ("line", 2, 2, 0), ("firstq", 2, 1), ("last", 2, 0, 0), ("line", 1, 2, 0),
    ("line", 3, 1, 1), ("last", 0, 1, 0), ("line", 2, 3, 0), ("line", 1, 1, 0), ("line", 1, 1, 1),
    ("last", 0, 2, 1), ("last", 0, 0, 0), ("last", 3, 0, 0), ("line", 1, 3, 0), ("last", 0, 0, 1),
    ("line", 1, 2, 1), ("firstq", 2, 0), ("last", 3, 0, 1), ("last", 0, 3, 0), ("last", 3, 3, 0),
    ("last", 0, 1, 1), ("last", 1, 0, 0), ("firstq", 2, 3), ("last", 3, 2, 1), ("last", 0, 3, 1),
    ("last", 3, 1, 0), ("firstq", 2, 2), ("line", 1, 3, 1), ("hidden", 0), ("last", 1, 0, 1),
    ("last", 3, 3, 1), ("down", 0, 0), ("down", 0, 1), ("last", 2, 1, 1), ("last", 3, 1, 1),
    ("last", 3, 2, 0), ("back", 0), ("last", 2, 2, 0), ("last", 2, 3, 0), ("hidden", 3), ("last", 2, 0, 1),
    ("last", 1, 2, 1), ("last", 2, 2, 1), ("last", 2, 3, 1), ("last", 2, 1, 0), ("down", 3, 0), ("hidden", 2),
    ("last", 1, 1, 0), ("down", 3, 1), ("fsum", 0, 0), ("back", 3), ("last", 1, 1, 1), ("last", 1, 3, 1),
    ("down", 2, 0), ("last", 1, 3, 0), ("down", 2, 1), ("last", 1, 2, 0), ("back", 2), ("hidden", 1),
    ("down", 1, 0), ("sum", 3, 0, 0), ("down", 1, 1), ("sum", 3, 0, 1), ("back", 1), ("sum", 3, 2, 0),
    ("sum", 3, 2, 1), ("sum", 1, 0, 0), ("sum", 3, 1, 0), ("fsum", 0, 2), ("fsum", 2, 0), ("sum", 1, 0, 1),
    ("sum", 3, 1, 1), ("fsum", 2, 2), ("zsum", 0, 0), ("sum", 1, 1, 0), ("fsum", 2, 3), ("sum", 1, 2, 1),
    ("sum", 1, 1, 1), ("fsum", 0, 1), ("fsum", 2, 1), ("zsum", 2, 0), ("fsum", 0, 3), ("sum", 1, 2, 0),
    ("home", 3, 1), ("zsum", 0, 1), ("zsum", 2, 2), ("home", 1, 1), ("zsum", 0, 2), ("zsum", 2, 1),
    ("home", 1, 0), ("final", 1), ("home", 3, 0), ("final", 3), ("homez", 0), ("drain_out", 0),
    ("drain_out", 1), ("drain_out", 2), ("drain_out", 3), ("drain_back", 0), ("drain_back", 1),
    ("drain_back", 3), ("homez", 2), ("drain_back", 2),
)

Z_FIRST_OUT = (True, False, True, False)
Z_LAST_BACK = (True, False, True, False)


def ring_kernel(
    zs, tok_ref, gain_ref, ids_ref, score_ref, prob_ref, gate_hbm, up_hbm, down_hbm, out_ref,
    xg, stage, part, pair_in, last_in, line_in, first_in, fin_in, hid, scales, wgu, wd, w_sem,
    stage_send, stage_recv, gather_recv, own_send, first_send, line_send, last_send,
    mate_send, mate_recv, pair_send, pair_recv, back_send, back_recv, sum_send, sum_recv,
    home_send, home_recv, fin_send, fin_recv,
):
    me = lax.axis_index("ep")
    core = lax.rem(me, 2)
    x = lax.rem(lax.div(me, 2), 2)
    y = lax.rem(lax.div(me, 4), 2)
    z = lax.div(me, 8)
    other = 1 - core

    def device(zz, yy, xx, cc):
        return ((zz * 2 + yy) * 2 + xx) * 2 + cc

    partner = device(z, y, x, other)
    first_dev = device(z, y + core * (1 - 2 * y), x + other * (1 - 2 * x), core)
    last_dev = device(z, y + other * (1 - 2 * y), x + core * (1 - 2 * x), core)
    has = (z > 0, z < zs - 1)

    def column(fr, lr):
        dx = other * fr + core * lr
        dy = core * fr + other * lr
        xx = x + dx * (1 - 2 * x)
        yy = y + dy * (1 - 2 * y)
        return (xx * 2 + yy) * zs

    cols = [[column(fr, lr) for lr in (0, 1)] for fr in (0, 1)]
    near = [sorted(range(zs), key=lambda q, zz=zz: (abs(q - zz), -q if zz < zs // 2 else q))
            for zz in range(zs)]
    planes = []
    for i in range(zs):
        q = jnp.int32(near[0][i])
        for zz in range(1, zs):
            q = jnp.where(z == zz, near[zz][i], q)
        planes.append(q)
    below = [q < z for q in planes]
    away = [jnp.where(b, z + 1, z - 1) for b in below]
    toward = [jnp.where(b, z - 1, z + 1) for b in below]
    side_of = [jnp.where(b, 1, 0) for b in below]

    model_width = tok_ref.shape[1]
    half = model_width // 2
    count = tok_ref.shape[0]
    rows = stage.shape[1]
    blocks = 4 * zs
    inner = hid.shape[2]

    copies = [
        pltpu.make_async_copy(gate_hbm.at[0], wgu.at[:, : wgu.shape[1] // 2], w_sem.at[0]),
        pltpu.make_async_copy(up_hbm.at[0], wgu.at[:, wgu.shape[1] // 2 :], w_sem.at[1]),
        pltpu.make_async_copy(down_hbm.at[0, :, :half], wd.at[0], w_sem.at[2]),
        pltpu.make_async_copy(down_hbm.at[0, :, half:], wd.at[1], w_sem.at[3]),
    ]
    for copy in copies:
        copy.start()

    barrier = pltpu.get_barrier_semaphore()
    for peer in (partner, first_dev, last_dev):
        pl.semaphore_signal(barrier, inc=1, device_id=(peer,), device_id_type=MESH)
    for d in (0, 1):
        @pl.when(has[d])
        def _():
            pl.semaphore_signal(
                barrier, inc=1, device_id=(device(z - 1 + 2 * d, y, x, core),), device_id_type=MESH
            )

    def remote(src, dst, send_sem, recv_sem, target):
        return pltpu.make_async_remote_copy(
            src_ref=src, dst_ref=dst, send_sem=send_sem, recv_sem=recv_sem,
            device_id=(target,), device_id_type=MESH,
        )

    def landed(ref, sem):
        remote(ref, ref, sem, sem, partner).wait_recv()

    def sent(ref, sem):
        remote(ref, ref, sem, sem, partner).wait_send()

    def wide(k):
        return half + LANES if k == 0 else half

    def block(h, k, slot):
        return xg.at[h, k, slot, :, pl.ds(0, wide(k))]

    def span(h, k, n):
        return xg.at[h, k, pl.ds(0, n), :, pl.ds(0, wide(k))]

    own_slot = cols[0][0] + z

    values = tok_ref[...].astype(jnp.float32)
    average = jnp.sum(values, axis=1, keepdims=True) * (1.0 / model_width)
    centred = values - average
    variance = jnp.sum(centred * centred, axis=1, keepdims=True) * (1.0 / model_width)
    normed = (centred * lax.rsqrt(variance + eps_norm) * gain_ref[...]).astype(jnp.bfloat16)
    for c in (0, 1):
        @pl.when(core == c)
        def _():
            for j in range(CHUNKS // 2):
                piece = normed[j * rows : (j + 1) * rows]
                mine = piece[:, :half] if c == 0 else piece[:, half:]
                theirs = piece[:, half:] if c == 0 else piece[:, :half]
                xg[c, 2 * j + c, own_slot, :, :half] = mine
                stage[j] = theirs
    score = [score_ref[k : k + 1, :] for k in range(TOP_K)]
    top = functools.reduce(jnp.maximum, score)
    exps = [jnp.exp(s - top) for s in score]
    total = functools.reduce(jnp.add, exps)
    row = lax.broadcasted_iota(jnp.int32, (rows, count), 0)
    tags = jnp.zeros((rows, count), jnp.float32)
    for k in range(TOP_K):
        weight = exps[k] / total * prob_ref[...]
        high = weight.astype(jnp.bfloat16).astype(jnp.float32)
        tags = jnp.where(row == k, ids_ref[k : k + 1, :].astype(jnp.float32), tags)
        tags = jnp.where(row == TOP_K + k, high, tags)
        tags = jnp.where(row == 2 * TOP_K + k, weight - high, tags)
    tags = jnp.concatenate([tags, jnp.zeros((rows, LANES - count), jnp.float32)], axis=1)
    xg[core, 0, own_slot, :, half:] = tags.astype(jnp.bfloat16)

    inside = jnp.logical_and(has[0], has[1])

    @pl.when(inside)
    def _():
        pl.semaphore_wait(barrier, 5)

    @pl.when(jnp.logical_not(inside))
    def _():
        pl.semaphore_wait(barrier, 4)

    for j in range(CHUNKS // 2):
        k = 2 * j + core
        remote(stage.at[j], xg.at[core * 0 + other, k, own_slot, :, pl.ds(0, half)],
               stage_send.at[j], stage_recv.at[k], partner).start()

    onward = jnp.where(z == 0, 1, z - 1)

    def program(at_end, order):
        sides = (jnp.where(z == 0, 1, 0),) if at_end else (0, 1)

        def out_z(ref, k, slot, sem_of):
            for n, d in enumerate((onward,) if at_end else (z - 1, z + 1)):
                remote(ref, ref, sem_of(n), gather_recv.at[k, slot], device(d, y, x, core)).start()

        def spread(k, fr, i):
            slot = cols[fr][0] + planes[i]
            ref = block(core, k, slot)
            sem = gather_recv.at[k, slot]
            if i == 0:
                out_z(ref, k, slot, lambda n: own_send.at[k, n])
            elif not at_end:
                remote(ref, ref, line_send.at[k, i], sem, device(away[i], y, x, core)).start()
            if Z_FIRST_OUT[k] and fr == 0:
                remote(ref, ref, first_send.at[k], sem, first_dev).start()
            remote(ref, ref, last_send.at[k], sem, last_dev).start()
            remote(ref, ref, mate_send.at[k], mate_recv.at[k], partner).start()

        def own(k):
            @pl.when(core != k % 2)
            def _():
                landed(xg.at[core, k, own_slot, :, pl.ds(0, half)], stage_recv.at[k])
            if not Z_FIRST_OUT[k]:
                ref = block(core, k, own_slot)
                remote(ref, ref, first_send.at[k], gather_recv.at[k, own_slot], first_dev).start()
            spread(k, 0, 0)

        def arrived(k, fr, lr, i):
            slot = cols[fr][lr] + planes[i]
            ref = block(core, k, slot)
            landed(ref, gather_recv.at[k, slot])
            return ref, slot

        def first(k):
            arrived(k, 1, 0, 0)
            spread(k, 1, 0)

        def line(k, i, fr):
            arrived(k, fr, 0, i)
            spread(k, fr, i)

        def firstq(k, i):
            ref, slot = arrived(k, 1, 0, i)
            remote(ref, ref, last_send.at[k], gather_recv.at[k, slot], last_dev).start()
            remote(ref, ref, mate_send.at[k], mate_recv.at[k], partner).start()

        def last(k, i, fr):
            ref, slot = arrived(k, fr, 1, i)
            remote(ref, ref, mate_send.at[k], mate_recv.at[k], partner).start()

        def hidden(k):
            landed(span(other, k, blocks), mate_recv.at[k])
            if order[[o[0] for o in order].index("hidden")][1] == k:
                start_compute()
            shape = (blocks, rows, LANES)
            pick = lax.broadcasted_iota(jnp.int32, shape, 2) == (
                lax.broadcasted_iota(jnp.int32, shape, 1) + rows * (k // 2))
            scale = jnp.sum(jnp.where(pick, scales[k % 2][:, None, :], 0.0), axis=2, keepdims=True)
            scale = scale.reshape(blocks * rows, 1)
            left = xg[0, k, :, :, :half].reshape(blocks * rows, half)
            right = xg[1, k, :, :, :half].reshape(blocks * rows, half)
            acts = jnp.dot(left, wgu[:half, :], preferred_element_type=jnp.float32) + jnp.dot(
                right, wgu[half:, :], preferred_element_type=jnp.float32
            )
            value = jax.nn.silu(acts[:, :inner]) * acts[:, inner:] * scale
            hid[k] = value.astype(jnp.bfloat16)

        def start_compute():
            for copy in copies:
                copy.wait()
            expert = me.astype(jnp.float32)
            for h in (0, 1):
                tags = xg[h, 0, :, :, half:].astype(jnp.float32)
                scale = jnp.zeros((blocks, LANES), jnp.float32)
                for n in range(TOP_K):
                    value = tags[:, TOP_K + n, :] + tags[:, 2 * TOP_K + n, :]
                    scale += jnp.where(tags[:, n, :] == expert, value, 0.0)
                scales[h] = scale

        def down(k, i):
            step = half // 3 if half % (3 * LANES) == 0 else half
            h = core if i else other
            for at in range(0, half, step):
                out = jnp.dot(hid[k], wd[h, :, at : at + step], preferred_element_type=jnp.float32)
                part[h, k, :, :, at : at + step] = out.astype(jnp.bfloat16).reshape(blocks, rows, step)
            if i == 0:
                remote(part.at[other, k], pair_in.at[k], pair_send.at[k], pair_recv.at[k], partner).start()

        def back(k):
            landed(pair_in.at[k], pair_recv.at[k])
            for i in range(zs - 1, -1, -1):
                for fr in (0, 1):
                    slot = cols[fr][1] + planes[i]
                    part[core, k, slot] = part[core, k, slot] + pair_in[k, slot]
                    remote(part.at[core, k, slot], last_in.at[k, fr, planes[i]], back_send.at[k],
                           back_recv.at[k, fr, planes[i]], last_dev).start()

        def collect(k, fr, q, from_line=(), from_first=False):
            slot = cols[fr][0] + q
            landed(last_in.at[k, fr, q], back_recv.at[k, fr, q])
            held = part[core, k, slot].astype(jnp.float32) + pair_in[k, slot].astype(jnp.float32)
            held = held + last_in[k, fr, q].astype(jnp.float32)
            if from_first:
                landed(first_in.at[k, q], home_recv.at[k, q])
                held = held + first_in[k, q].astype(jnp.float32)
            for side in from_line:
                landed(line_in.at[k, side, fr, q], sum_recv.at[k, side, fr, q])
                held = held + line_in[k, side, fr, q].astype(jnp.float32)
            part[core, k, slot] = held.astype(jnp.bfloat16)
            return slot

        def line_sum(k, j, fr):
            i = zs - 1 - j
            q = planes[i]
            slot = collect(k, fr, q, () if at_end else (side_of[i],), Z_LAST_BACK[k])
            remote(part.at[core, k, slot], line_in.at[k, side_of[i], fr, q], sum_send.at[k],
                   sum_recv.at[k, side_of[i], fr, q], device(toward[i], y, x, core)).start()

        def zsum(k, j):
            line_sum(k, j, 0)

        def to_first(k, slot, q):
            remote(part.at[core, k, slot], first_in.at[k, q], home_send.at[k], home_recv.at[k, q],
                   first_dev).start()

        def fsum(k, j):
            q = planes[zs - 1 - j]
            to_first(k, collect(k, 1, q), q)

        def home(k, fr):
            slot = collect(k, fr, z, sides)
            if fr == 1:
                to_first(k, slot, z)

        def finish(k, total):
            j = k // 2

            @pl.when(core == k % 2)
            def _():
                out_ref[j * rows : (j + 1) * rows, pl.ds(pl.multiple_of(core * half, LANES), half)] = total

            @pl.when(core != k % 2)
            def _():
                remote(part.at[core, k, own_slot], fin_in.at[j], fin_send.at[j], fin_recv.at[j],
                       partner).start()

        def final(k):
            landed(first_in.at[k, z], home_recv.at[k, z])
            total = part[core, k, own_slot] + first_in[k, z]
            part[core, k, own_slot] = total
            finish(k, total)

        def homez(k):
            collect(k, 0, z, sides, True)
            finish(k, part[core, k, own_slot])

        def drain_out(k):
            @pl.when(core == k % 2)
            def _():
                sent(stage.at[k // 2], stage_send.at[k // 2])
            wide_z = 1 if Z_FIRST_OUT[k] else 2
            sent(span(core, k, zs if Z_FIRST_OUT[k] else 1), first_send.at[k])
            for n in (0,) if at_end else (0, 1):
                sent(span(core, k, wide_z), own_send.at[k, n])
            for i in () if at_end else range(1, zs):
                sent(span(core, k, wide_z), line_send.at[k, i])
            sent(span(core, k, 2 * zs), last_send.at[k])
            sent(span(core, k, blocks), mate_send.at[k])

        def drain_back(k):
            sent(part.at[other, k], pair_send.at[k])
            sent(part.at[core, k, pl.ds(0, 2 * zs)], back_send.at[k])
            sent(part.at[core, k, pl.ds(0, (1 if Z_LAST_BACK[k] else 2) * (zs - 1))], sum_send.at[k])
            sent(part.at[core, k, pl.ds(0, zs if Z_LAST_BACK[k] else 1)], home_send.at[k])

        steps = dict(own=own, first=first, line=line, firstq=firstq, last=last, hidden=hidden, down=down,
                     back=back, sum=line_sum, zsum=zsum, fsum=fsum, home=home, homez=homez, final=final,
                     drain_out=drain_out, drain_back=drain_back)
        for name, *rest in order:
            steps[name](*rest)

    pl.when(inside)(lambda: program(False, INNER_ORDER))
    pl.when(jnp.logical_not(inside))(lambda: program(True, END_ORDER))

    for j in range(CHUNKS // 2):
        landed(fin_in.at[j], fin_recv.at[j])
        out_ref[j * rows : (j + 1) * rows, pl.ds(pl.multiple_of(other * half, LANES), half)] = fin_in[j]
    for j in range(CHUNKS // 2):
        sent(fin_in.at[j], fin_send.at[j])


def ring_local(
    zs, tokens, norm_gain, expert_ids, expert_scores, group_prob, gate_weight, up_weight, down_weight
):
    count, width = tokens.shape
    inner = gate_weight.shape[2]
    half = width // 2
    rows = 2 * count // CHUNKS
    blocks = 4 * zs
    kind = jnp.bfloat16
    vmem = pl.BlockSpec(memory_space=pltpu.VMEM)
    hbm = pl.BlockSpec(memory_space=pl.ANY)
    dma = pltpu.SemaphoreType.DMA
    c = CHUNKS
    scratch = [
        pltpu.VMEM((2, c, blocks, rows, half + LANES), kind),
        pltpu.VMEM((c // 2, rows, half), kind),
        pltpu.VMEM((2, c, blocks, rows, half), kind),
        pltpu.VMEM((c, blocks, rows, half), kind),
        pltpu.VMEM((c, 2, zs, rows, half), kind),
        pltpu.VMEM((c, 2, 2, zs, rows, half), kind),
        pltpu.VMEM((c, zs, rows, half), kind),
        pltpu.VMEM((c // 2, rows, half), kind),
        pltpu.VMEM((c, blocks * rows, inner), kind),
        pltpu.VMEM((2, blocks, LANES), jnp.float32),
        pltpu.VMEM((width, 2 * inner), kind),
        pltpu.VMEM((2, inner, half), kind),
        dma((4,)),
        dma((c // 2,)), dma((c,)), dma((c, blocks)), dma((c, 2)), dma((c,)), dma((c, zs)), dma((c,)),
        dma((c,)), dma((c,)), dma((c,)), dma((c,)), dma((c,)), dma((c, 2, zs)),
        dma((c,)), dma((c, 2, 2, zs)),
        dma((c,)), dma((c, zs)), dma((c // 2,)), dma((c // 2,)),
    ]
    return pl.pallas_call(
        functools.partial(ring_kernel, zs),
        out_shape=pltpu.VMEM((count, width), kind),
        in_specs=[vmem] * 5 + [hbm] * 3,
        out_specs=vmem,
        scratch_shapes=scratch,
        compiler_params=pltpu.CompilerParams(
            collective_id=0, has_side_effects=True, vmem_limit_bytes=60 * 1024 * 1024
        ),
    )(
        tokens, norm_gain[None, :], expert_ids.T, expert_scores.T, group_prob[None, :], gate_weight, up_weight, down_weight,
    )


def solution(mesh):
    in_specs = (
        P("ep", None),
        P(),
        P("ep", None),
        P("ep", None),
        P("ep"),
        P("ep", None, None),
        P("ep", None, None),
        P("ep", None, None),
    )
    out_specs = P("ep", None)
    devices = mesh.shape["ep"]
    body = functools.partial(ring_local, GROUPS) if devices == GROUPS * 8 else local
    return jax.shard_map(body, mesh=mesh, in_specs=in_specs, out_specs=out_specs, check_vma=False)
```

```python
import functools

import jax
import jax.numpy as jnp
from jax import lax
from jax.experimental import pallas as pl
from jax.experimental.pallas import tpu as pltpu
from jax.sharding import PartitionSpec as P

GROUPS = 4
TOP_K = 4
LANES = 128
MESH = pl.DeviceIdType.MESH


eps_norm = 1e-05


def layer_norm(tokens, norm_gain):
    values = tokens.astype(jnp.float32)
    average = jnp.mean(values, axis=1, keepdims=True)
    centred = values - average
    variance = jnp.mean(centred * centred, axis=1, keepdims=True)
    return (centred * lax.rsqrt(variance + eps_norm) * norm_gain[None, :]).astype(jnp.bfloat16)


def mixing_weights(expert_scores, group_prob):
    shifted = expert_scores - jnp.max(expert_scores, axis=1, keepdims=True)
    exp_scores = jnp.exp(shifted)
    return exp_scores / jnp.sum(exp_scores, axis=1, keepdims=True) * group_prob[:, None]


def expert_rows(flat_rows, gate_matrix, up_matrix, down_matrix):
    gate_act = jnp.dot(flat_rows, gate_matrix, preferred_element_type=jnp.float32)
    up_act = jnp.dot(flat_rows, up_matrix, preferred_element_type=jnp.float32)
    hidden = (jax.nn.silu(gate_act) * up_act).astype(jnp.bfloat16)
    return jnp.dot(hidden, down_matrix, preferred_element_type=jnp.float32).astype(jnp.bfloat16)


def local(
    tokens, norm_gain, expert_ids, expert_scores, group_prob, gate_weight, up_weight, down_weight
):
    normed = layer_norm(tokens, norm_gain)
    weights_tok = mixing_weights(expert_scores, group_prob)
    tok_count = tokens.shape[0]
    model_width = tokens.shape[1]
    expert_count = lax.axis_size("ep")
    group_size = expert_count // GROUPS
    capacity = (tok_count * TOP_K + group_size - 1) // group_size
    expert_iota = jnp.arange(expert_count, dtype=jnp.int32)
    slot_iota = jnp.arange(capacity, dtype=jnp.int32)
    matches = expert_ids[:, :, None] == expert_iota[None, None, :]
    route_weight = jnp.sum(jnp.where(matches, weights_tok[:, :, None], 0.0), axis=1)
    gate_matrix = gate_weight[0]
    up_matrix = up_weight[0]
    down_matrix = down_weight[0]
    chosen = jnp.sum(matches.astype(jnp.int32), axis=1)
    order_rank = jnp.cumsum(chosen, axis=0) - chosen
    slot_map = (chosen.T[:, None, :] == 1) & (order_rank.T[:, None, :] == slot_iota[None, :, None])
    outgoing = jnp.einsum(
        "emt,td->emd", slot_map.astype(jnp.bfloat16), normed, preferred_element_type=jnp.float32
    ).astype(jnp.bfloat16)
    received = lax.all_to_all(outgoing, "ep", split_axis=0, concat_axis=0, tiled=True)
    flat_rows = received.reshape(-1, model_width)
    results = expert_rows(flat_rows, gate_matrix, up_matrix, down_matrix).reshape(received.shape)
    returned_rows = lax.all_to_all(results, "ep", split_axis=0, concat_axis=0, tiled=True)
    slot_scale = jnp.where(slot_map, route_weight.T[:, None, :], 0.0)
    mixture = jnp.einsum(
        "emt,emd->td",
        slot_scale,
        returned_rows.astype(jnp.float32),
        precision=lax.Precision.HIGHEST,
    )
    return mixture.astype(jnp.bfloat16)

CHUNKS = 4


END_ORDER = (
    ("own", 0), ("own", 2), ("own", 1), ("line", 0, 1, 0), ("firstq", 0, 0), ("own", 3), ("first", 2),
    ("line", 1, 1, 0), ("line", 0, 2, 0), ("first", 3), ("line", 1, 2, 0), ("firstq", 0, 2),
    ("last", 3, 0, 0), ("last", 0, 0, 1), ("last", 0, 0, 0), ("firstq", 0, 1), ("line", 0, 3, 0),
    ("last", 1, 0, 0), ("last", 3, 0, 1), ("last", 0, 2, 0), ("last", 2, 0, 1), ("line", 1, 3, 0),
    ("last", 0, 1, 0), ("firstq", 0, 3), ("last", 1, 1, 0), ("firstq", 1, 1), ("last", 0, 1, 1),
    ("firstq", 1, 2), ("line", 2, 1, 1), ("last", 0, 3, 0), ("firstq", 1, 3), ("firstq", 1, 0),
    ("line", 2, 2, 1), ("last", 1, 3, 0), ("line", 2, 1, 0), ("last", 0, 2, 1), ("line", 2, 2, 0),
    ("line", 3, 3, 0), ("last", 0, 3, 1), ("line", 3, 1, 0), ("hidden", 0), ("last", 1, 2, 0),
    ("line", 2, 3, 0), ("line", 3, 2, 1), ("last", 1, 1, 1), ("last", 1, 3, 1), ("last", 1, 2, 1),
    ("last", 1, 0, 1), ("line", 2, 3, 1), ("last", 2, 1, 1), ("down", 0, 0), ("last", 2, 1, 0),
    ("down", 0, 1), ("line", 3, 3, 1), ("line", 3, 2, 0), ("line", 3, 1, 1), ("hidden", 1), ("last", 2, 2, 0),
    ("back", 0), ("last", 2, 2, 1), ("last", 2, 3, 1), ("last", 2, 0, 0), ("last", 3, 2, 1),
    ("last", 2, 3, 0), ("down", 1, 0), ("down", 1, 1), ("hidden", 2), ("last", 3, 1, 1), ("sum", 0, 0, 0),
    ("last", 3, 3, 1), ("last", 3, 2, 0), ("back", 1), ("last", 3, 3, 0), ("last", 3, 1, 0), ("down", 2, 0),
    ("down", 2, 1), ("sum", 0, 1, 0), ("hidden", 3), ("back", 2), ("sum", 0, 0, 1), ("sum", 0, 1, 1),
    ("sum", 1, 0, 0), ("sum", 1, 1, 1), ("down", 3, 0), ("sum", 1, 0, 1), ("sum", 1, 1, 0), ("sum", 0, 2, 0),
    ("sum", 1, 2, 1), ("sum", 0, 2, 1), ("down", 3, 1), ("back", 3), ("fsum", 3, 0), ("fsum", 2, 0),
    ("sum", 1, 2, 0), ("fsum", 3, 1), ("fsum", 2, 1), ("zsum", 3, 0), ("fsum", 3, 2), ("zsum", 2, 0),
    ("home", 1, 0), ("zsum", 2, 1), ("zsum", 3, 1), ("fsum", 2, 2), ("home", 1, 1), ("fsum", 3, 3),
    ("zsum", 2, 2), ("home", 0, 0), ("zsum", 3, 2), ("final", 1), ("home", 0, 1), ("fsum", 2, 3),
    ("homez", 3), ("homez", 2), ("drain_out", 0), ("drain_out", 1), ("drain_out", 2), ("drain_out", 3),
    ("drain_back", 1), ("drain_back", 2), ("drain_back", 3), ("final", 0), ("drain_back", 0),
)

INNER_ORDER = (
    ("own", 0), ("own", 2), ("own", 1), ("line", 0, 1, 0), ("line", 0, 2, 0), ("own", 3), ("line", 1, 2, 0),
    ("line", 1, 1, 0), ("line", 2, 2, 0), ("line", 0, 3, 0), ("line", 2, 1, 0), ("line", 1, 3, 0),
    ("line", 3, 2, 0), ("firstq", 0, 1), ("firstq", 0, 0), ("last", 1, 0, 0), ("firstq", 0, 2), ("first", 2),
    ("first", 3), ("firstq", 0, 3), ("line", 2, 2, 1), ("line", 3, 3, 0), ("line", 3, 2, 1),
    ("line", 2, 1, 1), ("last", 2, 2, 0), ("line", 3, 1, 1), ("line", 2, 3, 0), ("line", 2, 3, 1),
    ("last", 0, 1, 0), ("last", 0, 0, 0), ("last", 0, 2, 0), ("firstq", 1, 0), ("last", 3, 2, 0),
    ("last", 1, 1, 0), ("last", 2, 1, 0), ("line", 3, 1, 0), ("last", 0, 1, 1), ("last", 3, 0, 0),
    ("last", 0, 3, 0), ("last", 0, 2, 1), ("line", 3, 3, 1), ("last", 0, 0, 1), ("last", 1, 3, 0),
    ("last", 1, 2, 0), ("last", 0, 3, 1), ("hidden", 0), ("last", 3, 1, 1), ("last", 3, 2, 1),
    ("last", 3, 0, 1), ("firstq", 1, 3), ("last", 3, 3, 0), ("firstq", 1, 2), ("firstq", 1, 1),
    ("down", 0, 0), ("down", 0, 1), ("last", 1, 0, 1), ("last", 3, 3, 1), ("last", 3, 1, 0), ("back", 0),
    ("last", 2, 0, 0), ("last", 2, 0, 1), ("last", 1, 3, 1), ("last", 1, 2, 1), ("hidden", 3),
    ("last", 2, 1, 1), ("last", 1, 1, 1), ("last", 2, 2, 1), ("down", 3, 0), ("down", 3, 1), ("hidden", 1),
    ("back", 3), ("down", 1, 0), ("down", 1, 1), ("last", 2, 3, 0), ("last", 2, 3, 1), ("sum", 0, 0, 0),
    ("back", 1), ("hidden", 2), ("sum", 0, 0, 1), ("down", 2, 0), ("sum", 0, 2, 1), ("sum", 0, 2, 0),
    ("sum", 1, 0, 0), ("fsum", 3, 3), ("fsum", 3, 1), ("down", 2, 1), ("back", 2), ("sum", 1, 0, 1),
    ("sum", 1, 1, 0), ("fsum", 3, 0), ("fsum", 2, 0), ("sum", 1, 2, 0), ("sum", 1, 1, 1), ("fsum", 3, 2),
    ("fsum", 2, 1), ("sum", 1, 2, 1), ("sum", 0, 1, 0), ("sum", 0, 1, 1), ("zsum", 3, 0), ("zsum", 2, 0),
    ("fsum", 2, 2), ("home", 1, 1), ("zsum", 3, 2), ("zsum", 3, 1), ("fsum", 2, 3), ("home", 0, 1),
    ("zsum", 2, 1), ("zsum", 2, 2), ("home", 1, 0), ("final", 1), ("homez", 3), ("home", 0, 0), ("final", 0),
    ("drain_out", 0), ("drain_out", 1), ("drain_out", 2), ("drain_out", 3), ("drain_back", 0),
    ("drain_back", 1), ("drain_back", 3), ("homez", 2), ("drain_back", 2),
)

LOADS_AT = 12
Z_FIRST_OUT = (True, True, False, False)
Z_LAST_BACK = (False, False, True, True)


def ring_kernel(
    zs, tok_hbm, gain_hbm, ids_hbm, score_hbm, prob_hbm, gate_hbm, up_hbm, down_hbm, out_ref,
    tok_ref, gain_ref, ids_ref, score_ref, prob_ref, in_sem,
    xg, stage, part, pair_in, last_in, line_in, first_in, fin_in, hid, scales, wgu, wd, w_sem,
    stage_send, stage_recv, gather_recv, own_send, first_send, line_send, last_send,
    mate_send, mate_recv, pair_send, pair_recv, back_send, back_recv, sum_send, sum_recv,
    home_send, home_recv, fin_send, fin_recv,
):
    me = lax.axis_index("ep")
    core = lax.rem(me, 2)
    x = lax.rem(lax.div(me, 2), 2)
    y = lax.rem(lax.div(me, 4), 2)
    z = lax.div(me, 8)
    other = 1 - core

    def device(zz, yy, xx, cc):
        return ((zz * 2 + yy) * 2 + xx) * 2 + cc

    partner = device(z, y, x, other)
    first_dev = device(z, y + core * (1 - 2 * y), x + other * (1 - 2 * x), core)
    last_dev = device(z, y + other * (1 - 2 * y), x + core * (1 - 2 * x), core)
    has = (z > 0, z < zs - 1)

    def column(fr, lr):
        dx = other * fr + core * lr
        dy = core * fr + other * lr
        xx = x + dx * (1 - 2 * x)
        yy = y + dy * (1 - 2 * y)
        return (xx * 2 + yy) * zs

    cols = [[column(fr, lr) for lr in (0, 1)] for fr in (0, 1)]
    near = [sorted(range(zs), key=lambda q, zz=zz: (abs(q - zz), -q if zz < zs // 2 else q))
            for zz in range(zs)]
    planes = []
    for i in range(zs):
        q = jnp.int32(near[0][i])
        for zz in range(1, zs):
            q = jnp.where(z == zz, near[zz][i], q)
        planes.append(q)
    below = [q < z for q in planes]
    away = [jnp.where(b, z + 1, z - 1) for b in below]
    toward = [jnp.where(b, z - 1, z + 1) for b in below]
    side_of = [jnp.where(b, 1, 0) for b in below]

    model_width = tok_ref.shape[1]
    half = model_width // 2
    count = tok_ref.shape[0]
    rows = stage.shape[1]
    blocks = 4 * zs
    inner = hid.shape[2]

    tok_copies = [
        pltpu.make_async_copy(tok_hbm.at[pl.ds(j * rows, rows)], tok_ref.at[pl.ds(j * rows, rows)], in_sem.at[j])
        for j in range(CHUNKS // 2)
    ]
    small = [
        pltpu.make_async_copy(src, dst, in_sem.at[2 + i])
        for i, (src, dst) in enumerate(((gain_hbm, gain_ref), (ids_hbm, ids_ref), (score_hbm, score_ref), (prob_hbm, prob_ref)))
    ]
    for copy in (tok_copies[0], *small, tok_copies[1]):
        copy.start()

    barrier = pltpu.get_barrier_semaphore()
    for peer in (partner, first_dev, last_dev):
        pl.semaphore_signal(barrier, inc=1, device_id=(peer,), device_id_type=MESH)
    for d in (0, 1):
        @pl.when(has[d])
        def _():
            pl.semaphore_signal(
                barrier, inc=1, device_id=(device(z - 1 + 2 * d, y, x, core),), device_id_type=MESH
            )

    copies = [
        pltpu.make_async_copy(gate_hbm.at[0], wgu.at[:, : wgu.shape[1] // 2], w_sem.at[0]),
        pltpu.make_async_copy(up_hbm.at[0], wgu.at[:, wgu.shape[1] // 2 :], w_sem.at[1]),
        pltpu.make_async_copy(down_hbm.at[0, :, :half], wd.at[0], w_sem.at[2]),
        pltpu.make_async_copy(down_hbm.at[0, :, half:], wd.at[1], w_sem.at[3]),
    ]
    def remote(src, dst, send_sem, recv_sem, target):
        return pltpu.make_async_remote_copy(
            src_ref=src, dst_ref=dst, send_sem=send_sem, recv_sem=recv_sem,
            device_id=(target,), device_id_type=MESH,
        )

    def landed(ref, sem):
        remote(ref, ref, sem, sem, partner).wait_recv()

    def sent(ref, sem):
        remote(ref, ref, sem, sem, partner).wait_send()

    def wide(k):
        return half + LANES if k == 0 else half

    def block(h, k, slot):
        return xg.at[h, k, slot, :, pl.ds(0, wide(k))]

    def span(h, k, n):
        return xg.at[h, k, pl.ds(0, n), :, pl.ds(0, wide(k))]

    own_slot = cols[0][0] + z

    def normalize(j):
        values = tok_ref[j * rows : (j + 1) * rows].astype(jnp.float32)
        average = jnp.sum(values, axis=1, keepdims=True) * (1.0 / model_width)
        centred = values - average
        variance = jnp.sum(centred * centred, axis=1, keepdims=True) * (1.0 / model_width)
        piece = (centred * lax.rsqrt(variance + eps_norm) * gain_ref[...]).astype(jnp.bfloat16)
        for c in (0, 1):
            @pl.when(core == c)
            def _():
                mine = piece[:, :half] if c == 0 else piece[:, half:]
                theirs = piece[:, half:] if c == 0 else piece[:, :half]
                xg[c, 2 * j + c, own_slot, :, :half] = mine
                stage[j] = theirs

    def hand_over(j):
        remote(stage.at[j], xg.at[other, 2 * j + core, own_slot, :, pl.ds(0, half)],
               stage_send.at[j], stage_recv.at[2 * j + core], partner).start()

    small[0].wait()
    tok_copies[0].wait()
    normalize(0)
    inside = jnp.logical_and(has[0], has[1])

    @pl.when(inside)
    def _():
        pl.semaphore_wait(barrier, 5)

    @pl.when(jnp.logical_not(inside))
    def _():
        pl.semaphore_wait(barrier, 4)

    hand_over(0)
    for j in range(1, CHUNKS // 2):
        tok_copies[j].wait()
        normalize(j)
        hand_over(j)
    for copy in small[1:]:
        copy.wait()
    score = [score_ref[k : k + 1, :] for k in range(TOP_K)]
    top = functools.reduce(jnp.maximum, score)
    exps = [jnp.exp(s - top) for s in score]
    total = functools.reduce(jnp.add, exps)
    row = lax.broadcasted_iota(jnp.int32, (rows, count), 0)
    tags = jnp.zeros((rows, count), jnp.float32)
    for k in range(TOP_K):
        weight = exps[k] / total * prob_ref[...]
        high = weight.astype(jnp.bfloat16).astype(jnp.float32)
        tags = jnp.where(row == k, ids_ref[k : k + 1, :].astype(jnp.float32), tags)
        tags = jnp.where(row == TOP_K + k, high, tags)
        tags = jnp.where(row == 2 * TOP_K + k, weight - high, tags)
    tags = jnp.concatenate([tags, jnp.zeros((rows, LANES - count), jnp.float32)], axis=1)
    xg[core, 0, own_slot, :, half:] = tags.astype(jnp.bfloat16)


    onward = jnp.where(z == 0, 1, z - 1)

    def program(at_end, order):
        sides = (jnp.where(z == 0, 1, 0),) if at_end else (0, 1)

        def out_z(ref, k, slot, sem_of):
            for n, d in enumerate((onward,) if at_end else (z - 1, z + 1)):
                remote(ref, ref, sem_of(n), gather_recv.at[k, slot], device(d, y, x, core)).start()

        def spread(k, fr, i):
            slot = cols[fr][0] + planes[i]
            ref = block(core, k, slot)
            sem = gather_recv.at[k, slot]
            if i == 0:
                out_z(ref, k, slot, lambda n: own_send.at[k, n])
            elif not at_end:
                remote(ref, ref, line_send.at[k, i], sem, device(away[i], y, x, core)).start()
            if Z_FIRST_OUT[k] and fr == 0:
                remote(ref, ref, first_send.at[k], sem, first_dev).start()
            remote(ref, ref, last_send.at[k], sem, last_dev).start()
            remote(ref, ref, mate_send.at[k], mate_recv.at[k], partner).start()

        def own(k):
            @pl.when(core != k % 2)
            def _():
                landed(xg.at[core, k, own_slot, :, pl.ds(0, half)], stage_recv.at[k])
            if not Z_FIRST_OUT[k]:
                ref = block(core, k, own_slot)
                remote(ref, ref, first_send.at[k], gather_recv.at[k, own_slot], first_dev).start()
            spread(k, 0, 0)

        def arrived(k, fr, lr, i):
            slot = cols[fr][lr] + planes[i]
            ref = block(core, k, slot)
            landed(ref, gather_recv.at[k, slot])
            return ref, slot

        def first(k):
            arrived(k, 1, 0, 0)
            spread(k, 1, 0)

        def line(k, i, fr):
            arrived(k, fr, 0, i)
            spread(k, fr, i)

        def firstq(k, i):
            ref, slot = arrived(k, 1, 0, i)
            remote(ref, ref, last_send.at[k], gather_recv.at[k, slot], last_dev).start()
            remote(ref, ref, mate_send.at[k], mate_recv.at[k], partner).start()

        def last(k, i, fr):
            ref, slot = arrived(k, fr, 1, i)
            remote(ref, ref, mate_send.at[k], mate_recv.at[k], partner).start()

        def hidden(k):
            landed(span(other, k, blocks), mate_recv.at[k])
            if order[[o[0] for o in order].index("hidden")][1] == k:
                start_compute()
            shape = (blocks, rows, LANES)
            pick = lax.broadcasted_iota(jnp.int32, shape, 2) == (
                lax.broadcasted_iota(jnp.int32, shape, 1) + rows * (k // 2))
            scale = jnp.sum(jnp.where(pick, scales[k % 2][:, None, :], 0.0), axis=2, keepdims=True)
            scale = scale.reshape(blocks * rows, 1)
            left = xg[0, k, :, :, :half].reshape(blocks * rows, half)
            right = xg[1, k, :, :, :half].reshape(blocks * rows, half)
            acts = jnp.dot(left, wgu[:half, :], preferred_element_type=jnp.float32) + jnp.dot(
                right, wgu[half:, :], preferred_element_type=jnp.float32
            )
            value = jax.nn.silu(acts[:, :inner]) * acts[:, inner:] * scale
            hid[k] = value.astype(jnp.bfloat16)

        def start_compute():
            for copy in copies:
                copy.wait()
            expert = me.astype(jnp.float32)
            for h in (0, 1):
                tags = xg[h, 0, :, :, half:].astype(jnp.float32)
                scale = jnp.zeros((blocks, LANES), jnp.float32)
                for n in range(TOP_K):
                    value = tags[:, TOP_K + n, :] + tags[:, 2 * TOP_K + n, :]
                    scale += jnp.where(tags[:, n, :] == expert, value, 0.0)
                scales[h] = scale

        def down(k, i):
            step = half // 3 if half % (3 * LANES) == 0 else half
            h = core if i else other
            for at in range(0, half, step):
                out = jnp.dot(hid[k], wd[h, :, at : at + step], preferred_element_type=jnp.float32)
                part[h, k, :, :, at : at + step] = out.astype(jnp.bfloat16).reshape(blocks, rows, step)
            if i == 0:
                remote(part.at[other, k], pair_in.at[k], pair_send.at[k], pair_recv.at[k], partner).start()

        def back(k):
            landed(pair_in.at[k], pair_recv.at[k])
            for i in range(zs - 1, -1, -1):
                for fr in (0, 1):
                    slot = cols[fr][1] + planes[i]
                    part[core, k, slot] = part[core, k, slot] + pair_in[k, slot]
                    remote(part.at[core, k, slot], last_in.at[k, fr, planes[i]], back_send.at[k],
                           back_recv.at[k, fr, planes[i]], last_dev).start()

        def collect(k, fr, q, from_line=(), from_first=False):
            slot = cols[fr][0] + q
            landed(last_in.at[k, fr, q], back_recv.at[k, fr, q])
            held = part[core, k, slot].astype(jnp.float32) + pair_in[k, slot].astype(jnp.float32)
            held = held + last_in[k, fr, q].astype(jnp.float32)
            if from_first:
                landed(first_in.at[k, q], home_recv.at[k, q])
                held = held + first_in[k, q].astype(jnp.float32)
            for side in from_line:
                landed(line_in.at[k, side, fr, q], sum_recv.at[k, side, fr, q])
                held = held + line_in[k, side, fr, q].astype(jnp.float32)
            part[core, k, slot] = held.astype(jnp.bfloat16)
            return slot

        def line_sum(k, j, fr):
            i = zs - 1 - j
            q = planes[i]
            slot = collect(k, fr, q, () if at_end else (side_of[i],), Z_LAST_BACK[k])
            remote(part.at[core, k, slot], line_in.at[k, side_of[i], fr, q], sum_send.at[k],
                   sum_recv.at[k, side_of[i], fr, q], device(toward[i], y, x, core)).start()

        def zsum(k, j):
            line_sum(k, j, 0)

        def to_first(k, slot, q):
            remote(part.at[core, k, slot], first_in.at[k, q], home_send.at[k], home_recv.at[k, q],
                   first_dev).start()

        def fsum(k, j):
            q = planes[zs - 1 - j]
            to_first(k, collect(k, 1, q), q)

        def home(k, fr):
            slot = collect(k, fr, z, sides)
            if fr == 1:
                to_first(k, slot, z)

        def finish(k, total):
            j = k // 2

            @pl.when(core == k % 2)
            def _():
                out_ref[j * rows : (j + 1) * rows, pl.ds(pl.multiple_of(core * half, LANES), half)] = total

            @pl.when(core != k % 2)
            def _():
                remote(part.at[core, k, own_slot], fin_in.at[j], fin_send.at[j], fin_recv.at[j],
                       partner).start()

        def final(k):
            landed(first_in.at[k, z], home_recv.at[k, z])
            total = part[core, k, own_slot] + first_in[k, z]
            part[core, k, own_slot] = total
            finish(k, total)

        def homez(k):
            collect(k, 0, z, sides, True)
            finish(k, part[core, k, own_slot])

        def drain_out(k):
            @pl.when(core == k % 2)
            def _():
                sent(stage.at[k // 2], stage_send.at[k // 2])
            wide_z = 1 if Z_FIRST_OUT[k] else 2
            sent(span(core, k, zs if Z_FIRST_OUT[k] else 1), first_send.at[k])
            for n in (0,) if at_end else (0, 1):
                sent(span(core, k, wide_z), own_send.at[k, n])
            for i in () if at_end else range(1, zs):
                sent(span(core, k, wide_z), line_send.at[k, i])
            sent(span(core, k, 2 * zs), last_send.at[k])
            sent(span(core, k, blocks), mate_send.at[k])

        def drain_back(k):
            sent(part.at[other, k], pair_send.at[k])
            sent(part.at[core, k, pl.ds(0, 2 * zs)], back_send.at[k])
            sent(part.at[core, k, pl.ds(0, (1 if Z_LAST_BACK[k] else 2) * (zs - 1))], sum_send.at[k])
            sent(part.at[core, k, pl.ds(0, zs if Z_LAST_BACK[k] else 1)], home_send.at[k])

        steps = dict(own=own, first=first, line=line, firstq=firstq, last=last, hidden=hidden, down=down,
                     back=back, sum=line_sum, zsum=zsum, fsum=fsum, home=home, homez=homez, final=final,
                     drain_out=drain_out, drain_back=drain_back)
        for n, (name, *rest) in enumerate(order):
            if n == LOADS_AT:
                for copy in copies:
                    copy.start()
            steps[name](*rest)

    pl.when(inside)(lambda: program(False, INNER_ORDER))
    pl.when(jnp.logical_not(inside))(lambda: program(True, END_ORDER))

    for j in range(CHUNKS // 2):
        landed(fin_in.at[j], fin_recv.at[j])
        out_ref[j * rows : (j + 1) * rows, pl.ds(pl.multiple_of(other * half, LANES), half)] = fin_in[j]
    for j in range(CHUNKS // 2):
        sent(fin_in.at[j], fin_send.at[j])


def ring_local(
    zs, tokens, norm_gain, expert_ids, expert_scores, group_prob, gate_weight, up_weight, down_weight
):
    count, width = tokens.shape
    inner = gate_weight.shape[2]
    half = width // 2
    rows = 2 * count // CHUNKS
    blocks = 4 * zs
    kind = jnp.bfloat16
    vmem = pl.BlockSpec(memory_space=pltpu.VMEM)
    hbm = pl.BlockSpec(memory_space=pl.ANY)
    dma = pltpu.SemaphoreType.DMA
    c = CHUNKS
    scratch = [
        pltpu.VMEM((count, width), kind), pltpu.VMEM((1, width), jnp.float32),
        pltpu.VMEM((TOP_K, count), jnp.int32), pltpu.VMEM((TOP_K, count), jnp.float32),
        pltpu.VMEM((1, count), jnp.float32), dma((6,)),
        pltpu.VMEM((2, c, blocks, rows, half + LANES), kind),
        pltpu.VMEM((c // 2, rows, half), kind),
        pltpu.VMEM((2, c, blocks, rows, half), kind),
        pltpu.VMEM((c, blocks, rows, half), kind),
        pltpu.VMEM((c, 2, zs, rows, half), kind),
        pltpu.VMEM((c, 2, 2, zs, rows, half), kind),
        pltpu.VMEM((c, zs, rows, half), kind),
        pltpu.VMEM((c // 2, rows, half), kind),
        pltpu.VMEM((c, blocks * rows, inner), kind),
        pltpu.VMEM((2, blocks, LANES), jnp.float32),
        pltpu.VMEM((width, 2 * inner), kind),
        pltpu.VMEM((2, inner, half), kind),
        dma((4,)),
        dma((c // 2,)), dma((c,)), dma((c, blocks)), dma((c, 2)), dma((c,)), dma((c, zs)), dma((c,)),
        dma((c,)), dma((c,)), dma((c,)), dma((c,)), dma((c,)), dma((c, 2, zs)),
        dma((c,)), dma((c, 2, 2, zs)),
        dma((c,)), dma((c, zs)), dma((c // 2,)), dma((c // 2,)),
    ]
    return pl.pallas_call(
        functools.partial(ring_kernel, zs),
        out_shape=pltpu.VMEM((count, width), kind),
        in_specs=[hbm] * 8,
        out_specs=vmem,
        scratch_shapes=scratch,
        compiler_params=pltpu.CompilerParams(
            collective_id=0, has_side_effects=True, vmem_limit_bytes=60 * 1024 * 1024
        ),
    )(
        tokens, norm_gain[None, :], expert_ids.T, expert_scores.T, group_prob[None, :], gate_weight, up_weight, down_weight,
    )


def solution(mesh):
    in_specs = (
        P("ep", None),
        P(),
        P("ep", None),
        P("ep", None),
        P("ep"),
        P("ep", None, None),
        P("ep", None, None),
        P("ep", None, None),
    )
    out_specs = P("ep", None)
    devices = mesh.shape["ep"]
    body = functools.partial(ring_local, GROUPS) if devices == GROUPS * 8 else local
    return jax.shard_map(body, mesh=mesh, in_specs=in_specs, out_specs=out_specs, check_vma=False)
```

```python
import functools

import jax
import jax.numpy as jnp
from jax import lax
from jax.experimental import pallas as pl
from jax.experimental.pallas import tpu as pltpu
from jax.sharding import PartitionSpec as P

GROUPS = 4
TOP_K = 4
LANES = 128
MESH = pl.DeviceIdType.MESH


eps_norm = 1e-05


def layer_norm(tokens, norm_gain):
    values = tokens.astype(jnp.float32)
    average = jnp.mean(values, axis=1, keepdims=True)
    centred = values - average
    variance = jnp.mean(centred * centred, axis=1, keepdims=True)
    return (centred * lax.rsqrt(variance + eps_norm) * norm_gain[None, :]).astype(jnp.bfloat16)


def mixing_weights(expert_scores, group_prob):
    shifted = expert_scores - jnp.max(expert_scores, axis=1, keepdims=True)
    exp_scores = jnp.exp(shifted)
    return exp_scores / jnp.sum(exp_scores, axis=1, keepdims=True) * group_prob[:, None]


def expert_rows(flat_rows, gate_matrix, up_matrix, down_matrix):
    gate_act = jnp.dot(flat_rows, gate_matrix, preferred_element_type=jnp.float32)
    up_act = jnp.dot(flat_rows, up_matrix, preferred_element_type=jnp.float32)
    hidden = (jax.nn.silu(gate_act) * up_act).astype(jnp.bfloat16)
    return jnp.dot(hidden, down_matrix, preferred_element_type=jnp.float32).astype(jnp.bfloat16)


def local(
    tokens, norm_gain, expert_ids, expert_scores, group_prob, gate_weight, up_weight, down_weight
):
    normed = layer_norm(tokens, norm_gain)
    weights_tok = mixing_weights(expert_scores, group_prob)
    tok_count = tokens.shape[0]
    model_width = tokens.shape[1]
    expert_count = lax.axis_size("ep")
    group_size = expert_count // GROUPS
    capacity = (tok_count * TOP_K + group_size - 1) // group_size
    expert_iota = jnp.arange(expert_count, dtype=jnp.int32)
    slot_iota = jnp.arange(capacity, dtype=jnp.int32)
    matches = expert_ids[:, :, None] == expert_iota[None, None, :]
    route_weight = jnp.sum(jnp.where(matches, weights_tok[:, :, None], 0.0), axis=1)
    gate_matrix = gate_weight[0]
    up_matrix = up_weight[0]
    down_matrix = down_weight[0]
    chosen = jnp.sum(matches.astype(jnp.int32), axis=1)
    order_rank = jnp.cumsum(chosen, axis=0) - chosen
    slot_map = (chosen.T[:, None, :] == 1) & (order_rank.T[:, None, :] == slot_iota[None, :, None])
    outgoing = jnp.einsum(
        "emt,td->emd", slot_map.astype(jnp.bfloat16), normed, preferred_element_type=jnp.float32
    ).astype(jnp.bfloat16)
    received = lax.all_to_all(outgoing, "ep", split_axis=0, concat_axis=0, tiled=True)
    flat_rows = received.reshape(-1, model_width)
    results = expert_rows(flat_rows, gate_matrix, up_matrix, down_matrix).reshape(received.shape)
    returned_rows = lax.all_to_all(results, "ep", split_axis=0, concat_axis=0, tiled=True)
    slot_scale = jnp.where(slot_map, route_weight.T[:, None, :], 0.0)
    mixture = jnp.einsum(
        "emt,emd->td",
        slot_scale,
        returned_rows.astype(jnp.float32),
        precision=lax.Precision.HIGHEST,
    )
    return mixture.astype(jnp.bfloat16)

CHUNKS = 4


END_ORDER = (
    ("own", 0), ("own", 2), ("own", 1), ("line", 0, 1, 0), ("firstq", 0, 0), ("own", 3), ("first", 2),
    ("line", 1, 1, 0), ("line", 0, 2, 0), ("first", 3), ("line", 1, 2, 0), ("firstq", 0, 2),
    ("last", 3, 0, 0), ("last", 0, 0, 1), ("last", 0, 0, 0), ("firstq", 0, 1), ("line", 0, 3, 0),
    ("last", 1, 0, 0), ("last", 3, 0, 1), ("last", 0, 2, 0), ("last", 2, 0, 1), ("line", 1, 3, 0),
    ("last", 0, 1, 0), ("firstq", 0, 3), ("last", 1, 1, 0), ("firstq", 1, 1), ("last", 0, 1, 1),
    ("firstq", 1, 2), ("line", 2, 1, 1), ("last", 0, 3, 0), ("firstq", 1, 3), ("firstq", 1, 0),
    ("line", 2, 2, 1), ("last", 1, 3, 0), ("line", 2, 1, 0), ("last", 0, 2, 1), ("line", 2, 2, 0),
    ("line", 3, 3, 0), ("last", 0, 3, 1), ("line", 3, 1, 0), ("hidden", 0), ("last", 1, 2, 0),
    ("line", 2, 3, 0), ("line", 3, 2, 1), ("last", 1, 1, 1), ("last", 1, 3, 1), ("last", 1, 2, 1),
    ("last", 1, 0, 1), ("line", 2, 3, 1), ("last", 2, 1, 1), ("down", 0, 0), ("last", 2, 1, 0),
    ("down", 0, 1), ("line", 3, 3, 1), ("line", 3, 2, 0), ("line", 3, 1, 1), ("hidden", 1), ("last", 2, 2, 0),
    ("back", 0), ("last", 2, 2, 1), ("last", 2, 3, 1), ("last", 2, 0, 0), ("last", 3, 2, 1),
    ("last", 2, 3, 0), ("down", 1, 0), ("down", 1, 1), ("hidden", 2), ("last", 3, 1, 1), ("sum", 0, 0, 0),
    ("last", 3, 3, 1), ("last", 3, 2, 0), ("back", 1), ("last", 3, 3, 0), ("last", 3, 1, 0), ("down", 2, 0),
    ("down", 2, 1), ("sum", 0, 1, 0), ("hidden", 3), ("back", 2), ("sum", 0, 0, 1), ("sum", 0, 1, 1),
    ("sum", 1, 0, 0), ("sum", 1, 1, 1), ("down", 3, 0), ("sum", 1, 0, 1), ("sum", 1, 1, 0), ("sum", 0, 2, 0),
    ("sum", 1, 2, 1), ("sum", 0, 2, 1), ("down", 3, 1), ("back", 3), ("fsum", 3, 0), ("fsum", 2, 0),
    ("sum", 1, 2, 0), ("fsum", 3, 1), ("fsum", 2, 1), ("zsum", 3, 0), ("fsum", 3, 2), ("zsum", 2, 0),
    ("home", 1, 0), ("zsum", 2, 1), ("zsum", 3, 1), ("fsum", 2, 2), ("home", 1, 1), ("fsum", 3, 3),
    ("zsum", 2, 2), ("home", 0, 0), ("zsum", 3, 2), ("final", 1), ("home", 0, 1), ("fsum", 2, 3),
    ("homez", 3), ("homez", 2), ("drain_out", 0), ("drain_out", 1), ("drain_out", 2), ("drain_out", 3),
    ("drain_back", 1), ("drain_back", 2), ("drain_back", 3), ("final", 0), ("drain_back", 0),
)

INNER_ORDER = (
    ("own", 0), ("own", 2), ("own", 1), ("line", 0, 1, 0), ("line", 0, 2, 0), ("own", 3), ("line", 1, 2, 0),
    ("line", 1, 1, 0), ("line", 2, 2, 0), ("line", 0, 3, 0), ("line", 2, 1, 0), ("line", 1, 3, 0),
    ("line", 3, 2, 0), ("firstq", 0, 1), ("firstq", 0, 0), ("last", 1, 0, 0), ("firstq", 0, 2), ("first", 2),
    ("first", 3), ("firstq", 0, 3), ("line", 2, 2, 1), ("line", 3, 3, 0), ("line", 3, 2, 1),
    ("line", 2, 1, 1), ("last", 2, 2, 0), ("line", 3, 1, 1), ("line", 2, 3, 0), ("line", 2, 3, 1),
    ("last", 0, 1, 0), ("last", 0, 0, 0), ("last", 0, 2, 0), ("firstq", 1, 0), ("last", 3, 2, 0),
    ("last", 1, 1, 0), ("last", 2, 1, 0), ("line", 3, 1, 0), ("last", 0, 1, 1), ("last", 3, 0, 0),
    ("last", 0, 3, 0), ("last", 0, 2, 1), ("line", 3, 3, 1), ("last", 0, 0, 1), ("last", 1, 3, 0),
    ("last", 1, 2, 0), ("last", 0, 3, 1), ("hidden", 0), ("last", 3, 1, 1), ("last", 3, 2, 1),
    ("last", 3, 0, 1), ("firstq", 1, 3), ("last", 3, 3, 0), ("firstq", 1, 2), ("firstq", 1, 1),
    ("down", 0, 0), ("down", 0, 1), ("last", 1, 0, 1), ("last", 3, 3, 1), ("last", 3, 1, 0), ("back", 0),
    ("last", 2, 0, 0), ("last", 2, 0, 1), ("last", 1, 3, 1), ("last", 1, 2, 1), ("hidden", 3),
    ("last", 2, 1, 1), ("last", 1, 1, 1), ("last", 2, 2, 1), ("down", 3, 0), ("down", 3, 1), ("hidden", 1),
    ("back", 3), ("down", 1, 0), ("down", 1, 1), ("last", 2, 3, 0), ("last", 2, 3, 1), ("sum", 0, 0, 0),
    ("back", 1), ("hidden", 2), ("sum", 0, 0, 1), ("down", 2, 0), ("sum", 0, 2, 1), ("sum", 0, 2, 0),
    ("sum", 1, 0, 0), ("fsum", 3, 3), ("fsum", 3, 1), ("down", 2, 1), ("back", 2), ("sum", 1, 0, 1),
    ("sum", 1, 1, 0), ("fsum", 3, 0), ("fsum", 2, 0), ("sum", 1, 2, 0), ("sum", 1, 1, 1), ("fsum", 3, 2),
    ("fsum", 2, 1), ("sum", 1, 2, 1), ("sum", 0, 1, 0), ("sum", 0, 1, 1), ("zsum", 3, 0), ("zsum", 2, 0),
    ("fsum", 2, 2), ("home", 1, 1), ("zsum", 3, 2), ("zsum", 3, 1), ("fsum", 2, 3), ("home", 0, 1),
    ("zsum", 2, 1), ("zsum", 2, 2), ("home", 1, 0), ("final", 1), ("homez", 3), ("home", 0, 0), ("final", 0),
    ("drain_out", 0), ("drain_out", 1), ("drain_out", 2), ("drain_out", 3), ("drain_back", 0),
    ("drain_back", 1), ("drain_back", 3), ("homez", 2), ("drain_back", 2),
)

LOADS_AT = 12
Z_FIRST_OUT = (True, True, False, False)
Z_LAST_BACK = (False, False, True, True)


def ring_kernel(
    zs, tok_hbm, gain_hbm, ids_hbm, score_hbm, prob_hbm, gate_hbm, up_hbm, down_hbm, out_ref,
    tok_ref, gain_ref, ids_ref, score_ref, prob_ref, in_sem,
    xg, stage, part, pair_in, last_in, line_in, first_in, fin_in, hid, scales, wgu, wd, w_sem,
    stage_send, stage_recv, gather_recv, first_send, line_send, last_send,
    mate_send, mate_recv, pair_send, pair_recv, back_send, back_recv, sum_send, sum_recv,
    home_send, home_recv, fin_send, fin_recv,
):
    me = lax.axis_index("ep")
    core = lax.rem(me, 2)
    x = lax.rem(lax.div(me, 2), 2)
    y = lax.rem(lax.div(me, 4), 2)
    z = lax.div(me, 8)
    other = 1 - core

    def device(zz, yy, xx, cc):
        return ((zz * 2 + yy) * 2 + xx) * 2 + cc

    partner = device(z, y, x, other)
    first_dev = device(z, y + core * (1 - 2 * y), x + other * (1 - 2 * x), core)
    last_dev = device(z, y + other * (1 - 2 * y), x + core * (1 - 2 * x), core)
    has = (z > 0, z < zs - 1)

    def column(fr, lr):
        dx = other * fr + core * lr
        dy = core * fr + other * lr
        xx = x + dx * (1 - 2 * x)
        yy = y + dy * (1 - 2 * y)
        return (xx * 2 + yy) * zs

    cols = [[column(fr, lr) for lr in (0, 1)] for fr in (0, 1)]
    near = [sorted(range(zs), key=lambda q, zz=zz: (abs(q - zz), -q if zz < zs // 2 else q))
            for zz in range(zs)]
    planes = []
    for i in range(zs):
        q = jnp.int32(near[0][i])
        for zz in range(1, zs):
            q = jnp.where(z == zz, near[zz][i], q)
        planes.append(q)
    below = [q < z for q in planes]
    away = [jnp.where(b, z + 1, z - 1) for b in below]
    toward = [jnp.where(b, z - 1, z + 1) for b in below]
    side_of = [jnp.where(b, 1, 0) for b in below]

    model_width = tok_ref.shape[1]
    half = model_width // 2
    count = tok_ref.shape[0]
    rows = stage.shape[1]
    blocks = 4 * zs
    inner = hid.shape[2]

    tok_copies = [
        pltpu.make_async_copy(tok_hbm.at[pl.ds(j * rows, rows)], tok_ref.at[pl.ds(j * rows, rows)], in_sem.at[j])
        for j in range(CHUNKS // 2)
    ]
    small = [
        pltpu.make_async_copy(src, dst, in_sem.at[2 + i])
        for i, (src, dst) in enumerate(((gain_hbm, gain_ref), (ids_hbm, ids_ref), (score_hbm, score_ref), (prob_hbm, prob_ref)))
    ]
    for copy in (tok_copies[0], *small, tok_copies[1]):
        copy.start()

    barrier = pltpu.get_barrier_semaphore()
    for peer in (partner, first_dev, last_dev):
        pl.semaphore_signal(barrier, inc=1, device_id=(peer,), device_id_type=MESH)
    for d in (0, 1):
        @pl.when(has[d])
        def _():
            pl.semaphore_signal(
                barrier, inc=1, device_id=(device(z - 1 + 2 * d, y, x, core),), device_id_type=MESH
            )

    copies = [
        pltpu.make_async_copy(gate_hbm.at[0], wgu.at[:, : wgu.shape[1] // 2], w_sem.at[0]),
        pltpu.make_async_copy(up_hbm.at[0], wgu.at[:, wgu.shape[1] // 2 :], w_sem.at[1]),
        pltpu.make_async_copy(down_hbm.at[0, :, :half], wd.at[0], w_sem.at[2]),
        pltpu.make_async_copy(down_hbm.at[0, :, half:], wd.at[1], w_sem.at[3]),
    ]
    def remote(src, dst, send_sem, recv_sem, target):
        return pltpu.make_async_remote_copy(
            src_ref=src, dst_ref=dst, send_sem=send_sem, recv_sem=recv_sem,
            device_id=(target,), device_id_type=MESH,
        )

    def landed(ref, sem):
        remote(ref, ref, sem, sem, partner).wait_recv()

    def sent(ref, sem):
        remote(ref, ref, sem, sem, partner).wait_send()

    def wide(k):
        return half + LANES if k == 0 else half

    def block(h, k, slot):
        return xg.at[h, k, slot, :, pl.ds(0, wide(k))]

    def span(h, k, n):
        return xg.at[h, k, pl.ds(0, n), :, pl.ds(0, wide(k))]

    own_slot = cols[0][0] + z

    def normalize(j):
        values = tok_ref[j * rows : (j + 1) * rows].astype(jnp.float32)
        average = jnp.sum(values, axis=1, keepdims=True) * (1.0 / model_width)
        centred = values - average
        variance = jnp.sum(centred * centred, axis=1, keepdims=True) * (1.0 / model_width)
        piece = (centred * lax.rsqrt(variance + eps_norm) * gain_ref[...]).astype(jnp.bfloat16)
        for c in (0, 1):
            @pl.when(core == c)
            def _():
                mine = piece[:, :half] if c == 0 else piece[:, half:]
                theirs = piece[:, half:] if c == 0 else piece[:, :half]
                xg[c, 2 * j + c, own_slot, :, :half] = mine
                stage[j] = theirs

    def hand_over(j):
        remote(stage.at[j], xg.at[other, 2 * j + core, own_slot, :, pl.ds(0, half)],
               stage_send.at[j], stage_recv.at[2 * j + core], partner).start()

    small[0].wait()
    tok_copies[0].wait()
    normalize(0)
    inside = jnp.logical_and(has[0], has[1])

    @pl.when(inside)
    def _():
        pl.semaphore_wait(barrier, 5)

    @pl.when(jnp.logical_not(inside))
    def _():
        pl.semaphore_wait(barrier, 4)

    hand_over(0)
    for j in range(1, CHUNKS // 2):
        tok_copies[j].wait()
        normalize(j)
        hand_over(j)
    for copy in small[1:]:
        copy.wait()
    score = [score_ref[k : k + 1, :] for k in range(TOP_K)]
    top = functools.reduce(jnp.maximum, score)
    exps = [jnp.exp(s - top) for s in score]
    total = functools.reduce(jnp.add, exps)
    row = lax.broadcasted_iota(jnp.int32, (rows, count), 0)
    tags = jnp.zeros((rows, count), jnp.float32)
    for k in range(TOP_K):
        weight = exps[k] / total * prob_ref[...]
        high = weight.astype(jnp.bfloat16).astype(jnp.float32)
        tags = jnp.where(row == k, ids_ref[k : k + 1, :].astype(jnp.float32), tags)
        tags = jnp.where(row == TOP_K + k, high, tags)
        tags = jnp.where(row == 2 * TOP_K + k, weight - high, tags)
    tags = jnp.concatenate([tags, jnp.zeros((rows, LANES - count), jnp.float32)], axis=1)
    xg[core, 0, own_slot, :, half:] = tags.astype(jnp.bfloat16)


    onward = jnp.where(z == 0, 1, z - 1)

    def program(at_end, order):
        sides = (jnp.where(z == 0, 1, 0),) if at_end else (0, 1)

        def out_z(ref, k, slot, sem_of):
            for n, d in enumerate((onward,) if at_end else (z - 1, z + 1)):
                remote(ref, ref, sem_of(n), gather_recv.at[k, slot], device(d, y, x, core)).start()

        def spread(k, fr, i):
            slot = cols[fr][0] + planes[i]
            ref = block(core, k, slot)
            sem = gather_recv.at[k, slot]
            if i == 0:
                out_z(ref, k, slot, lambda n: line_send.at[k])
            elif not at_end:
                remote(ref, ref, line_send.at[k], sem, device(away[i], y, x, core)).start()
            if Z_FIRST_OUT[k] and fr == 0:
                remote(ref, ref, first_send.at[k], sem, first_dev).start()
            remote(ref, ref, last_send.at[k], sem, last_dev).start()
            remote(ref, ref, mate_send.at[k], mate_recv.at[k], partner).start()

        def own(k):
            @pl.when(core != k % 2)
            def _():
                landed(xg.at[core, k, own_slot, :, pl.ds(0, half)], stage_recv.at[k])
            if not Z_FIRST_OUT[k]:
                ref = block(core, k, own_slot)
                remote(ref, ref, first_send.at[k], gather_recv.at[k, own_slot], first_dev).start()
            spread(k, 0, 0)

        def arrived(k, fr, lr, i):
            slot = cols[fr][lr] + planes[i]
            ref = block(core, k, slot)
            landed(ref, gather_recv.at[k, slot])
            return ref, slot

        def first(k):
            arrived(k, 1, 0, 0)
            spread(k, 1, 0)

        def line(k, i, fr):
            arrived(k, fr, 0, i)
            spread(k, fr, i)

        def firstq(k, i):
            ref, slot = arrived(k, 1, 0, i)
            remote(ref, ref, last_send.at[k], gather_recv.at[k, slot], last_dev).start()
            remote(ref, ref, mate_send.at[k], mate_recv.at[k], partner).start()

        def last(k, i, fr):
            ref, slot = arrived(k, fr, 1, i)
            remote(ref, ref, mate_send.at[k], mate_recv.at[k], partner).start()

        def hidden(k):
            landed(span(other, k, blocks), mate_recv.at[k])
            if order[[o[0] for o in order].index("hidden")][1] == k:
                start_compute()
            shape = (blocks, rows, LANES)
            pick = lax.broadcasted_iota(jnp.int32, shape, 2) == (
                lax.broadcasted_iota(jnp.int32, shape, 1) + rows * (k // 2))
            scale = jnp.sum(jnp.where(pick, scales[k % 2][:, None, :], 0.0), axis=2, keepdims=True)
            scale = scale.reshape(blocks * rows, 1)
            left = xg[0, k, :, :, :half].reshape(blocks * rows, half)
            right = xg[1, k, :, :, :half].reshape(blocks * rows, half)
            acts = jnp.dot(left, wgu[:half, :], preferred_element_type=jnp.float32) + jnp.dot(
                right, wgu[half:, :], preferred_element_type=jnp.float32
            )
            value = jax.nn.silu(acts[:, :inner]) * acts[:, inner:] * scale
            hid[k] = value.astype(jnp.bfloat16)

        def start_compute():
            for copy in copies:
                copy.wait()
            expert = me.astype(jnp.float32)
            for h in (0, 1):
                tags = xg[h, 0, :, :, half:].astype(jnp.float32)
                scale = jnp.zeros((blocks, LANES), jnp.float32)
                for n in range(TOP_K):
                    value = tags[:, TOP_K + n, :] + tags[:, 2 * TOP_K + n, :]
                    scale += jnp.where(tags[:, n, :] == expert, value, 0.0)
                scales[h] = scale

        def down(k, i):
            step = half // 3 if half % (3 * LANES) == 0 else half
            h = core if i else other
            for at in range(0, half, step):
                out = jnp.dot(hid[k], wd[h, :, at : at + step], preferred_element_type=jnp.float32)
                part[h, k, :, :, at : at + step] = out.astype(jnp.bfloat16).reshape(blocks, rows, step)
            if i == 0:
                remote(part.at[other, k], pair_in.at[k], pair_send.at[k], pair_recv.at[k], partner).start()

        def back(k):
            landed(pair_in.at[k], pair_recv.at[k])
            for i in range(zs - 1, -1, -1):
                for fr in (0, 1):
                    slot = cols[fr][1] + planes[i]
                    part[core, k, slot] = part[core, k, slot] + pair_in[k, slot]
                    remote(part.at[core, k, slot], last_in.at[k, fr, planes[i]], back_send.at[k],
                           back_recv.at[k, fr, planes[i]], last_dev).start()

        def collect(k, fr, q, from_line=(), from_first=False):
            slot = cols[fr][0] + q
            landed(last_in.at[k, fr, q], back_recv.at[k, fr, q])
            held = part[core, k, slot].astype(jnp.float32) + pair_in[k, slot].astype(jnp.float32)
            held = held + last_in[k, fr, q].astype(jnp.float32)
            if from_first:
                landed(first_in.at[k, q], home_recv.at[k, q])
                held = held + first_in[k, q].astype(jnp.float32)
            for side in from_line:
                landed(line_in.at[k, side, fr, q], sum_recv.at[k, side, fr, q])
                held = held + line_in[k, side, fr, q].astype(jnp.float32)
            part[core, k, slot] = held.astype(jnp.bfloat16)
            return slot

        def line_sum(k, j, fr):
            i = zs - 1 - j
            q = planes[i]
            slot = collect(k, fr, q, () if at_end else (side_of[i],), Z_LAST_BACK[k])
            remote(part.at[core, k, slot], line_in.at[k, side_of[i], fr, q], sum_send.at[k],
                   sum_recv.at[k, side_of[i], fr, q], device(toward[i], y, x, core)).start()

        def zsum(k, j):
            line_sum(k, j, 0)

        def to_first(k, slot, q):
            remote(part.at[core, k, slot], first_in.at[k, q], home_send.at[k], home_recv.at[k, q],
                   first_dev).start()

        def fsum(k, j):
            q = planes[zs - 1 - j]
            to_first(k, collect(k, 1, q), q)

        def home(k, fr):
            slot = collect(k, fr, z, sides)
            if fr == 1:
                to_first(k, slot, z)

        def finish(k, total):
            j = k // 2

            @pl.when(core == k % 2)
            def _():
                out_ref[j * rows : (j + 1) * rows, pl.ds(pl.multiple_of(core * half, LANES), half)] = total

            @pl.when(core != k % 2)
            def _():
                remote(part.at[core, k, own_slot], fin_in.at[j], fin_send.at[j], fin_recv.at[j],
                       partner).start()

        def final(k):
            landed(first_in.at[k, z], home_recv.at[k, z])
            total = part[core, k, own_slot] + first_in[k, z]
            part[core, k, own_slot] = total
            finish(k, total)

        def homez(k):
            collect(k, 0, z, sides, True)
            finish(k, part[core, k, own_slot])

        def drain_out(k):
            @pl.when(core == k % 2)
            def _():
                sent(stage.at[k // 2], stage_send.at[k // 2])
            wide_z = 1 if Z_FIRST_OUT[k] else 2
            sent(span(core, k, zs if Z_FIRST_OUT[k] else 1), first_send.at[k])
            sent(span(core, k, wide_z * (1 if at_end else zs + 1)), line_send.at[k])
            sent(span(core, k, 2 * zs), last_send.at[k])
            sent(span(core, k, blocks), mate_send.at[k])

        def drain_back(k):
            sent(part.at[other, k], pair_send.at[k])
            sent(part.at[core, k, pl.ds(0, 2 * zs)], back_send.at[k])
            sent(part.at[core, k, pl.ds(0, (1 if Z_LAST_BACK[k] else 2) * (zs - 1))], sum_send.at[k])
            sent(part.at[core, k, pl.ds(0, zs if Z_LAST_BACK[k] else 1)], home_send.at[k])

        steps = dict(own=own, first=first, line=line, firstq=firstq, last=last, hidden=hidden, down=down,
                     back=back, sum=line_sum, zsum=zsum, fsum=fsum, home=home, homez=homez, final=final,
                     drain_out=drain_out, drain_back=drain_back)
        for n, (name, *rest) in enumerate(order):
            if n == LOADS_AT:
                for copy in copies:
                    copy.start()
            steps[name](*rest)

    pl.when(inside)(lambda: program(False, INNER_ORDER))
    pl.when(jnp.logical_not(inside))(lambda: program(True, END_ORDER))

    for j in range(CHUNKS // 2):
        landed(fin_in.at[j], fin_recv.at[j])
        out_ref[j * rows : (j + 1) * rows, pl.ds(pl.multiple_of(other * half, LANES), half)] = fin_in[j]
    for j in range(CHUNKS // 2):
        sent(fin_in.at[j], fin_send.at[j])


def ring_local(
    zs, tokens, norm_gain, expert_ids, expert_scores, group_prob, gate_weight, up_weight, down_weight
):
    count, width = tokens.shape
    inner = gate_weight.shape[2]
    half = width // 2
    rows = 2 * count // CHUNKS
    blocks = 4 * zs
    kind = jnp.bfloat16
    vmem = pl.BlockSpec(memory_space=pltpu.VMEM)
    hbm = pl.BlockSpec(memory_space=pl.ANY)
    dma = pltpu.SemaphoreType.DMA
    c = CHUNKS
    scratch = [
        pltpu.VMEM((count, width), kind), pltpu.VMEM((1, width), jnp.float32),
        pltpu.VMEM((TOP_K, count), jnp.int32), pltpu.VMEM((TOP_K, count), jnp.float32),
        pltpu.VMEM((1, count), jnp.float32), dma((6,)),
        pltpu.VMEM((2, c, blocks, rows, half + LANES), kind),
        pltpu.VMEM((c // 2, rows, half), kind),
        pltpu.VMEM((2, c, blocks, rows, half), kind),
        pltpu.VMEM((c, blocks, rows, half), kind),
        pltpu.VMEM((c, 2, zs, rows, half), kind),
        pltpu.VMEM((c, 2, 2, zs, rows, half), kind),
        pltpu.VMEM((c, zs, rows, half), kind),
        pltpu.VMEM((c // 2, rows, half), kind),
        pltpu.VMEM((c, blocks * rows, inner), kind),
        pltpu.VMEM((2, blocks, LANES), jnp.float32),
        pltpu.VMEM((width, 2 * inner), kind),
        pltpu.VMEM((2, inner, half), kind),
        dma((4,)),
        dma((c // 2,)), dma((c,)), dma((c, blocks)), dma((c,)), dma((c,)), dma((c,)),
        dma((c,)), dma((c,)), dma((c,)), dma((c,)), dma((c,)), dma((c, 2, zs)),
        dma((c,)), dma((c, 2, 2, zs)),
        dma((c,)), dma((c, zs)), dma((c // 2,)), dma((c // 2,)),
    ]
    return pl.pallas_call(
        functools.partial(ring_kernel, zs),
        out_shape=pltpu.VMEM((count, width), kind),
        in_specs=[hbm] * 8,
        out_specs=vmem,
        scratch_shapes=scratch,
        compiler_params=pltpu.CompilerParams(
            collective_id=0, has_side_effects=True, vmem_limit_bytes=60 * 1024 * 1024
        ),
    )(
        tokens, norm_gain[None, :], expert_ids.T, expert_scores.T, group_prob[None, :], gate_weight, up_weight, down_weight,
    )


def solution(mesh):
    in_specs = (
        P("ep", None),
        P(),
        P("ep", None),
        P("ep", None),
        P("ep"),
        P("ep", None, None),
        P("ep", None, None),
        P("ep", None, None),
    )
    out_specs = P("ep", None)
    devices = mesh.shape["ep"]
    body = functools.partial(ring_local, GROUPS) if devices == GROUPS * 8 else local
    return jax.shard_map(body, mesh=mesh, in_specs=in_specs, out_specs=out_specs, check_vma=False)
```
